512 devices in a mesh: sp: 64 (over z, y), tp: 8 (over x, core).
Axes of the slice: x: 4, y: 8, z: 8, core: 2. Of those that a mesh axis runs over, the one named last changes fastest.
Arguments:
- tokens: bfloat16 [65536, 2048], P(('sp', 'tp')), may hold values from -6 to 6
- norm_gain: float32 [2048], replicated, may hold values from 0.1 to 1.9
- w_query: bfloat16 [2048, 2048], P('sp', 'tp'), may hold values from -0.125 to 0.125
- w_key: bfloat16 [2048, 2048], P('sp', 'tp'), may hold values from -0.125 to 0.125
- w_value: bfloat16 [2048, 4096], P('sp', 'tp'), may hold values from -0.125 to 0.125
- w_rank_down: bfloat16 [2048, 16], replicated, may hold values from -0.125 to 0.125
- w_rank_up: bfloat16 [16, 2048], P(None, 'tp'), may hold values from -1.5 to 1.5
- gate_bias: float32 [2048], P('tp')
- decay_shift: float32 [65536], P('sp'), may hold values from -1 to 0
- out_gain: float32 [512], replicated, may hold values from 0.1 to 1.9
- w_out: bfloat16 [4096, 2048], P('tp', 'sp'), may hold values from -0.09375 to 0.09375
Outputs:
- mixed: bfloat16 [65536, 2048], P(('sp', 'tp'))
The draws below stay inside these ranges and needn't reach their ends.
All inputs are finite; a program needn't handle non-finite values.
Results may differ from the reference program's by a relative error of at most 0.015.
Values may be sent and summed in bfloat16 or wider, within the bound.
A program may use at most 128 MiB of HBM per device.

```python
import jax
import jax.numpy as jnp
from jax import lax

D = 2048
HEADS = 8
DK = 256
DV = 512
RANK = 16
TAU = 16
BLOCK = 64
STRETCH = 1024
TOKENS = 65536
KEYS = 2048
VALS = 4096
N_SP = 64
N_TP = 8


def draw_gate_bias(key, part):
    first, second, third = jax.random.split(key, 3)
    share = 0.5
    slow_head = jax.random.uniform(first, (HEADS,)) < share
    slow = jnp.log(2.0 * TOKENS / TAU) + jax.random.uniform(second, (HEADS, DK), minval=-0.5, maxval=0.5)
    fast = jax.random.uniform(third, (HEADS, DK), minval=0.5, maxval=1.5)
    return jnp.where(slow_head[:, None], slow, fast).reshape(HEADS * DK).astype(jnp.float32)


def draw_decay_shift(key, part):
    first, second, third, fourth = jax.random.split(key, 4)
    stretches = TOKENS // STRETCH
    level = jnp.exp(jax.random.uniform(first, (stretches,), minval=jnp.log(0.1), maxval=0.0))
    spread = jax.random.uniform(second, (TOKENS,), minval=0.5, maxval=1.5)
    per_position = -jnp.repeat(level, STRETCH) * spread / TOKENS
    spots = jax.random.randint(third, (3,), 0, TOKENS)
    drops = jnp.log(jax.random.uniform(fourth, (3,), minval=0.5, maxval=0.8))
    return per_position.at[spots].add(drops).astype(jnp.float32)


def shard_levels(stream_key, dims, cuts, least, top_value):
    def one(axis_at, parts):
        steps = jax.random.uniform(jax.random.fold_in(jax.random.fold_in(stream_key, 6), axis_at), (parts,), jnp.float32, least / len(cuts), top_value / len(cuts))
        return jnp.repeat(jnp.exp(steps), dims[axis_at] // parts).reshape((-1,) + (1,) * (len(dims) - axis_at - 1))

    factor_of = one(*cuts[0])
    for cut in cuts[1:]:
        factor_of = factor_of * one(*cut)
    return factor_of


def noise(own_key, extent, deviation, most, cuts=(), kind=jnp.bfloat16):
    array = deviation * jax.random.normal(own_key, extent, jnp.float32)
    if cuts:
        array = array * shard_levels(own_key, extent, cuts, -0.22, 0.18)
    return jnp.clip(array, -most, most).astype(kind)


def setup_inputs(seed: int = 0) -> dict:
    splits = jax.random.split(jax.random.key(seed), 12)
    tokens = noise(splits[0], (TOKENS, D), 1.0, 6.0, ((0, 512),))
    norm_gain = jnp.clip(1.0 + 0.18 * jax.random.normal(splits[1], (D,), jnp.float32), 0.1, 1.9)
    w_query = noise(splits[2], (D, KEYS), D ** -0.5, 0.125, ((0, 64), (1, 8)))
    w_key = noise(splits[3], (D, KEYS), D ** -0.5, 0.125, ((0, 64), (1, 8)))
    w_value = noise(splits[4], (D, VALS), D ** -0.5, 0.125, ((0, 64), (1, 8)))
    w_rank_down = noise(splits[5], (D, RANK), D ** -0.5, 0.125)
    w_rank_up = noise(splits[6], (RANK, KEYS), RANK ** -0.5, 1.5, ((1, 8),))
    gate_bias = draw_gate_bias(jax.random.fold_in(splits[11], 71), 0)
    decay_shift = draw_decay_shift(jax.random.fold_in(splits[11], 71), 0)
    out_gain = jnp.clip(1.0 + 0.18 * jax.random.normal(splits[9], (DV,), jnp.float32), 0.1, 1.9)
    w_out = noise(splits[10], (VALS, D), VALS ** -0.5, 0.09375, ((0, 8), (1, 64)))
    return dict(tokens=tokens, norm_gain=norm_gain, w_query=w_query, w_key=w_key, w_value=w_value, w_rank_down=w_rank_down, w_rank_up=w_rank_up, gate_bias=gate_bias, decay_shift=decay_shift, out_gain=out_gain, w_out=w_out)


EPS = 1e-06

def rms_rows(values, gain):
    wide = values.astype(jnp.float32)
    return wide * lax.rsqrt(lax.optimization_barrier(jnp.mean(wide * wide, axis=-1, keepdims=True)) + EPS) * gain

def narrow(values):
    return lax.optimization_barrier(values.astype(jnp.bfloat16)).astype(jnp.float32)

def local_pass(query, key, value, log_decay, state):
    rows, heads, width = query.shape
    blocks = rows // BLOCK

    def split(tensor):
        return tensor.reshape((blocks, BLOCK) + tensor.shape[1:])
    causal = jnp.tril(jnp.ones((BLOCK, BLOCK), dtype=bool))

    def step(carry, inputs):
        q_blk, k_blk, v_blk, g_blk = inputs
        cumul = jnp.cumsum(g_blk, axis=0)
        centre = cumul - cumul[BLOCK // 2]
        q_scaled = narrow(q_blk * jnp.exp(centre))
        k_scaled = narrow(k_blk * jnp.exp(-centre))
        scores = jnp.einsum('ihd,jhd->hij', q_scaled, k_scaled)
        scores = narrow(jnp.where(causal[None], scores, 0.0))
        within = jnp.einsum('hij,jhe->ihe', scores, v_blk)
        final = cumul[-1]
        decayed = narrow(k_blk * jnp.exp(final - cumul))
        nxt = jnp.exp(final)[:, :, None] * carry + jnp.einsum('jhd,jhe->hde', decayed, v_blk)
        return (nxt, (within, q_blk * jnp.exp(cumul), final, carry))
    carry, (within, reach, finals, starts) = lax.scan(step, state, (split(query), split(key), split(value), split(log_decay)))
    return (within, reach, finals, starts, carry)

def read_out(reach, starts):
    blocks, block, heads, width = reach.shape
    result = jnp.einsum('nihd,nhde->nihe', narrow(reach), narrow(starts))
    return result.reshape(blocks * block, heads, -1)

def reference(tokens, norm_gain, w_query, w_key, w_value, w_rank_down, w_rank_up, gate_bias, decay_shift, out_gain, w_out):
    group_width = HEADS // N_TP * DV

    def segment(state, inputs):
        rows, shift = inputs
        normed = rms_rows(rows, norm_gain).astype(jnp.bfloat16)
        query = jnp.dot(normed, w_query, preferred_element_type=jnp.float32).astype(jnp.bfloat16)
        keyed = jnp.dot(normed, w_key, preferred_element_type=jnp.float32).astype(jnp.bfloat16)
        valued = jnp.dot(normed, w_value, preferred_element_type=jnp.float32).astype(jnp.bfloat16)
        rank = jnp.dot(normed, w_rank_down, preferred_element_type=jnp.float32).astype(jnp.bfloat16)
        pre = jnp.dot(rank, w_rank_up, preferred_element_type=jnp.float32) + gate_bias
        log_decay = jax.nn.log_sigmoid(pre) / TAU + shift[:, None]
        q_heads = query.astype(jnp.float32).reshape(STRETCH, HEADS, DK) * DK ** (-0.5)
        k_heads = keyed.astype(jnp.float32).reshape(STRETCH, HEADS, DK)
        v_heads = valued.astype(jnp.float32).reshape(STRETCH, HEADS, DV)
        within, reach, _, starts, state = local_pass(q_heads, k_heads, v_heads, log_decay.reshape(STRETCH, HEADS, DK), state)
        attended = within.reshape(STRETCH, HEADS, DV) + read_out(reach, starts)
        shaped = rms_rows(attended, out_gain).astype(jnp.bfloat16).reshape(STRETCH, VALS)
        total = jnp.zeros((STRETCH, D), jnp.float32)
        for group in range(N_TP):
            lower = group * group_width
            part = jnp.dot(shaped[:, lower:lower + group_width], w_out[lower:lower + group_width], preferred_element_type=jnp.float32).astype(jnp.bfloat16)
            total = total + lax.optimization_barrier(part).astype(jnp.float32)
        return (state, total.astype(jnp.bfloat16))
    start = jnp.zeros((HEADS, DK, DV), jnp.float32)
    _, mixed = lax.scan(segment, start, (tokens.reshape(N_SP, STRETCH, D), decay_shift.reshape(N_SP, STRETCH)))
    return mixed.reshape(TOKENS, D)
```

```python
import jax
import jax.numpy as jnp
from jax import lax
from jax.experimental import pallas as pl
from jax.experimental.pallas import tpu as pltpu
from jax.sharding import Mesh
from jax.sharding import PartitionSpec as P

DK = 256
DV = 512
TAU = 16
BLOCK = 64
QUAD = 256
SP = ("sp_0", "sp_1")
SP_TP = ("sp_0", "sp_1", "tp")
EPS = 1e-06
VMEM = pl.BlockSpec(memory_space=pltpu.VMEM)


def sent_together(arrays, axis, dim, along):
    both = jnp.concatenate(arrays, axis=along)
    out, at, finished = (lax.all_gather(both, axis, axis=dim, tiled=True), 0, [])
    for a in arrays:
        finished.append(lax.slice_in_dim(out, at, at + a.shape[along], axis=along))
        at += a.shape[along]
    return tuple(finished)


def filled_with(value, identity):
    return jax.tree.map(
        lambda a, e: jnp.broadcast_to(jnp.asarray(e, a.dtype), a.shape), value, identity
    )


def entering(value, axes, combine, identity):
    before = start = filled_with(value, identity)
    total = value
    for axis in reversed(axes):
        size, mine = (lax.axis_size(axis), lax.axis_index(axis))
        pieces = jax.tree.map(lambda part: lax.all_gather(part, axis), total)
        inside, total = (start, start)
        for k in range(size):
            passed = k < mine
            total = combine(total, jax.tree.map(lambda part: part[k], pieces))
            inside = jax.tree.map(lambda new, old: jnp.where(passed, new, old), total, inside)
        before = combine(inside, before)
    return before


def cut_along(value, dim, size):
    before, after = (value.shape[:dim], value.shape[dim + 1 :])
    return jnp.moveaxis(value.reshape(*before, size, -1, *after), dim, 0)


def sent_and_summed(value, axis, dim):
    size = lax.axis_size(axis)
    parts = lax.all_to_all(cut_along(value, dim, size), axis, 0, 0, tiled=True)
    return jnp.sum(parts.astype(jnp.float32), axis=0)


def rms_rows(values, gain):
    wide = values.astype(jnp.float32)
    return wide * lax.rsqrt(jnp.mean(wide * wide, axis=-1, keepdims=True) + EPS) * gain


def combine(earlier, later):
    return (earlier[0] * later[0], later[0][None, :] * earlier[1] + later[1])


def dot(a, b, dims):
    return lax.dot_general(a, b, (dims, ((), ())), preferred_element_type=jnp.float32)


NN, NT, TN = (((1,), (0,)), ((1,), (1,)), ((0,), (0,)))


def block_masks():
    row = lax.broadcasted_iota(jnp.int32, (QUAD, QUAD), 0)
    col = lax.broadcasted_iota(jnp.int32, (QUAD, QUAD), 1)
    return (row // BLOCK == col // BLOCK) & (col <= row)


def local_kernel(x_ref, up_ref, bias_ref, shift_ref, att_ref, far_ref, state_ref, total_ref):
    rows = x_ref.shape[0]
    state_ref[...] = jnp.zeros_like(state_ref)
    total_ref[...] = jnp.zeros_like(total_ref)
    nb = QUAD // BLOCK

    def body(i, carry):
        at = pl.ds(pl.multiple_of(i * QUAD, QUAD), QUAD)
        causal = block_masks()
        lower = jnp.where(causal, 1.0, 0.0).astype(jnp.bfloat16)
        pre = dot(x_ref[at, 1024:1040], up_ref[...], NN) + bias_ref[...]
        logs = jnp.minimum(pre, 0.0) - jnp.log1p(jnp.exp(-jnp.abs(pre)))
        decay = logs * (1.0 / TAU) + shift_ref[at, :]
        hi = decay.astype(jnp.bfloat16)
        rest = decay - hi.astype(jnp.float32)
        mid = rest.astype(jnp.bfloat16)
        low = (rest - mid.astype(jnp.float32)).astype(jnp.bfloat16)
        cumul = dot(lower, hi, NN) + (dot(lower, mid, NN) + dot(lower, low, NN))
        cube = cumul.reshape(nb, BLOCK, DK)
        middle, final = (cube[:, BLOCK // 2 : BLOCK // 2 + 1], cube[:, BLOCK - 1 : BLOCK])
        centre = (cube - middle).reshape(QUAD, DK)
        tail = (final - cube).reshape(QUAD, DK)
        q = x_ref[at, 0:DK].astype(jnp.float32) * DK ** (-0.5)
        k = x_ref[at, DK : 2 * DK].astype(jnp.float32)
        q_scaled = (q * jnp.exp(centre)).astype(jnp.bfloat16)
        k_scaled = (k * jnp.exp(-centre)).astype(jnp.bfloat16)
        reach = q * jnp.exp(cumul)
        decayed = (k * jnp.exp(tail)).astype(jnp.bfloat16)
        v = x_ref[at, 2 * DK : 2 * DK + DV]
        scores = jnp.where(causal, dot(q_scaled, k_scaled, NT), 0.0).astype(jnp.bfloat16)
        within = dot(scores, v, NN)
        for n in range(nb):
            part = slice(n * BLOCK, (n + 1) * BLOCK)
            base = total_ref[...]
            rows_at = pl.ds(pl.multiple_of(i * QUAD + n * BLOCK, BLOCK), BLOCK)
            far_ref[rows_at, :] = (reach[part] * jnp.exp(base)).astype(jnp.bfloat16)
            state = state_ref[...]
            read = dot(reach[part].astype(jnp.bfloat16), state.astype(jnp.bfloat16), NT)
            att_ref[rows_at, :] = within[part] + read
            state_ref[...] = jnp.exp(final[n]) * state + dot(v[part], decayed[part], TN)
            total_ref[...] = base + final[n]
        return carry

    lax.fori_loop(0, rows // QUAD, body, 0)


def finish_kernel(att_ref, far_ref, carried_ref, gain_ref, out_w_ref, part_ref):
    rows = att_ref.shape[0]

    def body(i, carry):
        at = pl.ds(pl.multiple_of(i * QUAD, QUAD), QUAD)
        att = att_ref[at, :] + dot(far_ref[at, :], carried_ref[...], NT)
        shaped = att * lax.rsqrt(jnp.mean(att * att, axis=-1, keepdims=True) + EPS) * gain_ref[...]
        part_ref[at, :] = dot(shaped.astype(jnp.bfloat16), out_w_ref[...], NN).astype(jnp.bfloat16)
        return carry

    lax.fori_loop(0, rows // QUAD, body, 0)


def on_device(
    tokens,
    norm_gain,
    w_query,
    w_key,
    w_value,
    w_rank_down,
    w_rank_up,
    gate_bias,
    decay_shift,
    out_gain,
    w_out,
):
    normed = rms_rows(tokens, norm_gain).astype(jnp.bfloat16)
    query_w, key_w, value_w = sent_together((w_query, w_key, w_value), SP, 0, 1)
    w_joined = jnp.concatenate([query_w, key_w, value_w, w_rank_down], axis=1)
    joined = jnp.dot(
        lax.all_gather(normed, "tp", axis=0, tiled=True),
        w_joined,
        preferred_element_type=jnp.float32,
    ).astype(jnp.bfloat16)
    span = joined.shape[0]
    att, far, local_end, total = pl.pallas_call(
        local_kernel,
        out_shape=(
            jax.ShapeDtypeStruct((span, DV), jnp.float32),
            jax.ShapeDtypeStruct((span, DK), jnp.bfloat16),
            jax.ShapeDtypeStruct((DV, DK), jnp.float32),
            jax.ShapeDtypeStruct((1, DK), jnp.float32),
        ),
        in_specs=[VMEM] * 4,
        out_specs=(VMEM,) * 4,
    )(joined, w_rank_up, gate_bias[None], decay_shift[:, None])
    identity = (jnp.ones((DK,), jnp.float32), jnp.zeros((DV, DK), jnp.float32))
    carried = entering((jnp.exp(total[0]), local_end), SP, combine, identity)[1]
    out_whole = lax.all_gather(w_out, SP, axis=1, tiled=True)
    partial = pl.pallas_call(
        finish_kernel,
        out_shape=jax.ShapeDtypeStruct((span, out_whole.shape[1]), jnp.bfloat16),
        in_specs=[VMEM] * 5,
        out_specs=VMEM,
    )(att, far, carried.astype(jnp.bfloat16), out_gain[None], out_whole)
    return sent_and_summed(partial, "tp", 0).astype(jnp.bfloat16)


def solution(mesh):
    finer = Mesh(mesh.devices.reshape(8, 8, mesh.shape["tp"]), ("sp_0", "sp_1", "tp"))
    in_specs = (
        P(SP_TP, None),
        P(),
        P(SP, "tp"),
        P(SP, "tp"),
        P(SP, "tp"),
        P(),
        P(None, "tp"),
        P("tp"),
        P(SP),
        P(),
        P("tp", SP),
    )
    out_specs = P(SP_TP, None)
    return jax.shard_map(
        on_device, mesh=finer, in_specs=in_specs, out_specs=out_specs, check_vma=False
    )
```

```python
import jax
import jax.numpy as jnp
from jax import lax
from jax.experimental import pallas as pl
from jax.experimental.pallas import tpu as pltpu
from jax.sharding import Mesh
from jax.sharding import PartitionSpec as P

DK = 256
DV = 512
TAU = 16
BLOCK = 64
QUAD = 256
D = 2048
EPS = 1e-06
NY = NZ = 8
NX = 4
SP = ("z", "y")
TP = ("x", "c")
ALL = ("z", "y", "x", "c")
MESH = pl.DeviceIdType.MESH
VMEM = pl.BlockSpec(memory_space=pltpu.VMEM)
BF16 = jnp.bfloat16
F32 = jnp.float32
NN, NT, TN = (((1,), (0,)), ((1,), (1,)), ((0,), (0,)))


def dot(a, b, dims):
    return lax.dot_general(a, b, (dims, ((), ())), preferred_element_type=F32)


def block_masks():
    row = lax.broadcasted_iota(jnp.int32, (QUAD, QUAD), 0)
    col = lax.broadcasted_iota(jnp.int32, (QUAD, QUAD), 1)
    return (row // BLOCK == col // BLOCK) & (col <= row)


def split3(value):
    hi = value.astype(BF16)
    rest = value - hi.astype(F32)
    mid = rest.astype(BF16)
    low = (rest - mid.astype(F32)).astype(BF16)
    return hi, mid, low


def remote(src, dst, send, recv, **device):
    return pltpu.make_async_remote_copy(
        src_ref=src, dst_ref=dst, send_sem=send, recv_sem=recv, device_id=device, device_id_type=MESH
    )


class Spread:
    def __init__(self, buf, at, rows, first, send, recv):
        self.buf, self.rows, self.send, self.recv = buf, rows, send, recv
        self.first, self.second = first, "z" if first == "y" else "y"
        self.at = at
        self.where = {"y": lax.axis_index("y"), "z": lax.axis_index("z")}

    def rest(self):
        return (pl.ds(self.at, self.rows), slice(None))

    def shard(self, along):
        pos = dict(self.where)
        pos[self.first] = along
        return self.buf.at[(pos["z"], pos["y"]) + self.rest()]

    def half(self, line, h):
        part = pl.ds(4 * h, 4)
        lead = (line, part) if self.second == "z" else (part, line)
        return self.buf.at[lead + self.rest()]

    def push(self, d):
        mine = self.where[self.first]
        ref = self.shard(mine)
        return remote(ref, ref, self.send.at[d - 1], self.recv.at[d - 1], **{self.first: lax.rem(mine + d, 8)})

    def start_push(self):
        for d in (1, 7, 2, 6, 3, 5, 4):
            self.push(d).start()

    def wait_push(self):
        mine = self.where[self.first]
        for d in (1, 7, 2, 6, 3, 5, 4):
            ref = self.shard(lax.rem(mine - d + 8, 8))
            remote(ref, ref, self.send.at[d - 1], self.recv.at[d - 1], **{self.first: mine}).wait_recv()

    def hop(self, s, h, way):
        mine = self.where[self.second]
        step = 1 if way == 0 else 7
        line = lax.rem(mine + (8 - step) * (s - 1), 8)
        ref = self.half(line, h)
        i = 7 + way * 7 + 2 * (s - 1) + (h if s < 4 else 0)
        return remote(ref, ref, self.send.at[i], self.recv.at[i], **{self.second: lax.rem(mine + step, 8)})

    def wait_hop(self, s, h, way):
        mine = self.where[self.second]
        step = 1 if way == 0 else 7
        ref = self.half(lax.rem(mine + (8 - step) * s, 8), h)
        i = 7 + way * 7 + 2 * (s - 1) + (h if s < 4 else 0)
        remote(ref, ref, self.send.at[i], self.recv.at[i], **{self.second: mine}).wait_recv()

    def hops(self, s):
        if s < 4:
            return [(0, 0), (1, 1), (1, 0), (0, 1)]
        return [(0, 0), (1, 1)]

    def finish(self):
        self.wait_hop(3, 1, 0)
        self.wait_hop(3, 0, 1)
        self.wait_hop(4, 0, 0)
        self.wait_hop(4, 1, 1)

    def drain(self):
        for d in range(1, 8):
            self.push(d).wait_send()
        for s in range(1, 5):
            for h, way in self.hops(s):
                self.hop(s, h, way).wait_send()


def relay(pieces, s):
    for k in range(4 if s < 4 else 2):
        for p in pieces:
            h, way = p.hops(s)[k]
            if s > 1:
                p.wait_hop(s - 1, h, way)
            p.hop(s, h, way).start()


def layer_kernel(
    tok_ref,
    gain_ref,
    wq_ref,
    wk_ref,
    wv_ref,
    down_ref,
    up_ref,
    bias_ref,
    shift_ref,
    ogain_ref,
    wo_ref,
    out_ref,
    xn,
    wqk,
    wv,
    wo,
    att_ref,
    far_ref,
    state_ref,
    total_ref,
    give,
    decay_out,
    got,
    decays,
    answer,
    carried,
    part,
    other,
    chip,
    ring_l,
    ring_r,
    from_l,
    from_r,
    tok_send,
    tok_recv,
    w_send,
    w_recv,
    scan_send,
    scan_recv,
    rs_send,
    rs_recv,
):
    z, y, x, c = (lax.axis_index(a) for a in ALL)
    sp = z * NY + y
    right, left, mate = lax.rem(x + 1, NX), lax.rem(x + NX - 1, NX), 1 - c

    def peer(d):
        p = lax.rem(sp + d, 64)
        return {"z": lax.div(p, 8), "y": lax.rem(p, 8)}

    barrier = pltpu.get_barrier_semaphore()

    def greet(d, carry):
        pl.semaphore_signal(barrier, inc=1, device_id=peer(d), device_id_type=MESH)
        return carry

    pl.semaphore_signal(barrier, inc=1, device_id={"x": right}, device_id_type=MESH)
    pl.semaphore_signal(barrier, inc=1, device_id={"x": left}, device_id_type=MESH)
    pl.semaphore_signal(barrier, inc=1, device_id={"c": mate}, device_id_type=MESH)
    lax.fori_loop(1, 64, greet, 0)

    wv[z, y] = wv_ref[...]
    wqk[z, y, :, 0:DK] = wq_ref[...]
    wqk[z, y, :, DK : 2 * DK] = wk_ref[...]
    wo[z, y] = wo_ref[...].astype(F32).T.astype(BF16)
    for h in range(2):
        rows = slice(64 * h, 64 * h + 64)
        wide = tok_ref[rows, :].astype(F32)
        normed = wide * lax.rsqrt(jnp.mean(wide * wide, axis=-1, keepdims=True) + EPS) * gain_ref[...]
        xn[x, c, rows, :] = normed.astype(BF16)

    pl.semaphore_wait(barrier, 66)

    value = Spread(wv, 0, 32, "y", w_send.at[0], w_recv.at[0])
    qk = Spread(wqk, 0, 32, "z", w_send.at[1], w_recv.at[1])
    out_a = Spread(wo, 0, 16, "y", w_send.at[2], w_recv.at[2])
    out_b = Spread(wo, 16, 16, "z", w_send.at[3], w_recv.at[3])
    value.start_push()
    qk.start_push()

    def rows_of(xx, h):
        return xn.at[xx, c, pl.ds(64 * h, 64), :]

    def token(i, xx, h, to):
        ref = rows_of(xx, h)
        return remote(ref, ref, tok_send.at[i], tok_recv.at[i], x=to)

    def to_mate(i, xx, h):
        ref = rows_of(xx, h)
        return remote(ref, ref, tok_send.at[i], tok_recv.at[i], c=mate)

    far_x = lax.rem(x + 2, NX)
    sends = [token(0, x, 0, right), token(3, x, 1, left), token(1, x, 1, right), token(4, x, 0, left)]
    for s in sends:
        s.start()
    shares = [to_mate(6, x, 0), to_mate(7, x, 1)]
    for s in shares:
        s.start()

    def arrive(i, xx, h, slot):
        token(i, xx, h, x).wait_recv()
        share = to_mate(slot, xx, h)
        share.start()
        shares.append(share)

    value.wait_push()
    qk.wait_push()
    relay((value, qk), 1)
    arrive(0, left, 0, 8)
    sends.append(token(2, left, 0, right))
    sends[-1].start()
    arrive(3, right, 1, 9)
    sends.append(token(5, right, 1, left))
    sends[-1].start()
    relay((value, qk), 2)
    arrive(1, left, 1, 10)
    arrive(4, right, 0, 11)
    relay((value, qk), 3)
    arrive(2, far_x, 0, 12)
    arrive(5, far_x, 1, 13)
    relay((value, qk), 4)
    out_a.start_push()
    out_b.start_push()
    value.finish()
    qk.finish()
    for i, xx, h in [
        (6, x, 0),
        (7, x, 1),
        (8, left, 0),
        (9, right, 1),
        (10, left, 1),
        (11, right, 0),
        (12, far_x, 0),
        (13, far_x, 1),
    ]:
        ref = xn.at[xx, mate, pl.ds(64 * h, 64), :]
        remote(ref, ref, tok_send.at[i], tok_recv.at[i], c=mate).wait_recv()

    state_ref[...] = jnp.zeros_like(state_ref)
    total_ref[...] = jnp.zeros_like(total_ref)
    nb = QUAD // BLOCK

    def quad(i, carry):
        for s in range(1, 5):

            @pl.when(i == s - 1)
            def _():
                if s == 1:
                    out_a.wait_push()
                    out_b.wait_push()
                relay((out_a, out_b), s)

        at = pl.ds(pl.multiple_of(i * QUAD, QUAD), QUAD)
        rows = xn[i].reshape(QUAD, D)
        joined = dot(rows, wqk[...].reshape(D, 2 * DK), NN).astype(BF16)
        v = dot(rows, wv[...].reshape(D, DV), NN).astype(BF16)
        rank = dot(rows, down_ref[...], NN).astype(BF16)
        causal = block_masks()
        lower = jnp.where(causal, 1.0, 0.0).astype(BF16)
        pre = dot(rank, up_ref[...], NN) + bias_ref[...]
        logs = jnp.minimum(pre, 0.0) - jnp.log1p(jnp.exp(-jnp.abs(pre)))
        ones = jnp.ones((8, DK), BF16)
        shift = shift_ref[pl.ds(i, 1), :]
        shifts = sum(dot(jnp.broadcast_to(t.astype(F32), (8, QUAD)).astype(BF16), ones, TN) for t in split3(shift)) * 0.125
        decay = logs * (1.0 / TAU) + shifts
        hi, mid, low = split3(decay)
        cumul = dot(lower, hi, NN) + (dot(lower, mid, NN) + dot(lower, low, NN))
        cube = cumul.reshape(nb, BLOCK, DK)
        middle, final = (cube[:, BLOCK // 2 : BLOCK // 2 + 1], cube[:, BLOCK - 1 : BLOCK])
        centre = (cube - middle).reshape(QUAD, DK)
        tail = (final - cube).reshape(QUAD, DK)
        q = joined[:, 0:DK].astype(F32) * DK ** (-0.5)
        k = joined[:, DK : 2 * DK].astype(F32)
        q_scaled = (q * jnp.exp(centre)).astype(BF16)
        k_scaled = (k * jnp.exp(-centre)).astype(BF16)
        reach = q * jnp.exp(cumul)
        decayed = (k * jnp.exp(tail)).astype(BF16)
        scores = jnp.where(causal, dot(q_scaled, k_scaled, NT), 0.0).astype(BF16)
        within = dot(scores, v, NN)
        for n in range(nb):
            cut = slice(n * BLOCK, (n + 1) * BLOCK)
            base = total_ref[...]
            rows_at = pl.ds(pl.multiple_of(i * QUAD + n * BLOCK, BLOCK), BLOCK)
            far_ref[rows_at, :] = (reach[cut] * jnp.exp(base)).astype(BF16)
            state = state_ref[...]
            read = dot(reach[cut].astype(BF16), state.astype(BF16), NT)
            att_ref[rows_at, :] = within[cut] + read
            state_ref[...] = jnp.exp(final[n]) * state + dot(v[cut], decayed[cut], TN)
            total_ref[...] = base + final[n]
        return carry

    lax.fori_loop(0, NX, quad, 0)

    give[...] = state_ref[...].reshape(64, 8, DK).astype(BF16)
    decay_out[...] = jnp.exp(total_ref[...])
    got[sp] = give[sp]
    decays[sp] = decay_out[...]

    def ask(d):
        j = lax.rem(sp + d, 64)
        return (
            remote(give.at[j], got.at[sp], scan_send.at[0], scan_recv.at[0], **peer(d)),
            remote(decay_out, decays.at[sp], scan_send.at[1], scan_recv.at[1], **peer(d)),
        )

    def reply(d):
        j = lax.rem(sp + d, 64)
        return remote(answer.at[j], carried.at[sp], scan_send.at[2], scan_recv.at[2], **peer(d))

    def start_ask(d, carry):
        for r in ask(d):
            r.start()
        return carry

    def start_reply(d, carry):
        reply(d).start()
        return carry

    def wait_all(ref, sem):
        most = ref.at[pl.ds(0, 63)]
        pltpu.make_async_copy(most, most, sem).wait()

    lax.fori_loop(1, 64, start_ask, 0)
    wait_all(got, scan_recv.at[0])
    wait_all(decays, scan_recv.at[1])

    def prefix(j, carry):
        answer[j] = carry.astype(BF16)
        return decays[j] * carry + got[j].astype(F32)

    lax.fori_loop(0, 64, prefix, jnp.zeros((8, DK), F32))
    carried[sp] = answer[sp]
    lax.fori_loop(1, 64, start_reply, 0)
    out_a.finish()
    out_b.finish()
    wait_all(carried, scan_recv.at[2])

    halves = (pl.ds(0, 64), pl.ds(64, 64))

    def swap(k):
        return remote(part.at[k, mate], other.at[k], rs_send.at[k], rs_recv.at[k], c=mate)

    def ring(i, src, dst, to):
        return remote(src, dst, rs_send.at[4 + i], rs_recv.at[4 + i], x=to)

    hops = (
        ring(0, chip.at[0, halves[0]], ring_l, right),
        ring(1, chip.at[0, halves[1]], ring_r, left),
        ring(2, chip.at[1, halves[1]], from_l.at[halves[1]], right),
        ring(3, chip.at[2, halves[0]], from_r.at[halves[0]], left),
        ring(4, chip.at[1, halves[0]], from_l.at[halves[0]], right),
        ring(5, chip.at[2, halves[1]], from_r.at[halves[1]], left),
    )

    def both(k, rows):
        return part[k, c, rows, :].astype(F32) + other[k, rows, :].astype(F32)

    def finish(k, carry):
        off = jnp.where(k == 0, 2, jnp.where(k == 1, 1, jnp.where(k == 2, 3, 0)))
        to = lax.rem(x + off, NX)
        at = pl.ds(pl.multiple_of(to * QUAD, QUAD), QUAD)
        att = att_ref[at, :] + dot(far_ref[at, :], carried[...].reshape(DV, DK), NT)
        shaped = att * lax.rsqrt(jnp.mean(att * att, axis=-1, keepdims=True) + EPS) * ogain_ref[...]
        res = dot(shaped.astype(BF16), wo[...].reshape(D, DV), NT).astype(BF16)
        part[k] = res.reshape(2, 128, D)
        swap(k).start()

        @pl.when(k == 1)
        def _():
            swap(0).wait_recv()
            chip[0] = both(0, slice(None)).astype(BF16)
            hops[0].start()
            hops[1].start()

        @pl.when(k == 2)
        def _():
            swap(1).wait_recv()
            chip[1, halves[1], :] = both(1, halves[1]).astype(BF16)
            hops[2].start()

        @pl.when(k == 3)
        def _():
            swap(2).wait_recv()
            chip[2, halves[0], :] = both(2, halves[0]).astype(BF16)
            hops[3].start()

        return carry

    lax.fori_loop(0, NX, finish, 0)
    hops[0].wait_recv()
    chip[1, halves[0], :] = (both(1, halves[0]) + ring_l[...].astype(F32)).astype(BF16)
    hops[4].start()
    hops[1].wait_recv()
    chip[2, halves[1], :] = (both(2, halves[1]) + ring_r[...].astype(F32)).astype(BF16)
    hops[5].start()
    swap(3).wait_recv()
    for i in (2, 3, 4, 5):
        hops[i].wait_recv()
    out_ref[...] = (both(3, slice(None)) + from_l[...].astype(F32) + from_r[...].astype(F32)).astype(BF16)

    for s in sends + shares:
        s.wait_send()
    for p in (value, qk, out_a, out_b):
        p.drain()
    sent = give.at[pl.ds(0, 63)]
    pltpu.make_async_copy(sent, sent, scan_send.at[0]).wait()
    wait_all(decays, scan_send.at[1])
    wait_all(answer, scan_send.at[2])
    for k in range(4):
        swap(k).wait_send()
    for h in hops:
        h.wait_send()


def on_device(
    tokens,
    norm_gain,
    w_query,
    w_key,
    w_value,
    w_rank_down,
    w_rank_up,
    gate_bias,
    decay_shift,
    out_gain,
    w_out,
):
    return pl.pallas_call(
        layer_kernel,
        out_shape=jax.ShapeDtypeStruct(tokens.shape, BF16),
        in_specs=[VMEM] * 11,
        out_specs=VMEM,
        scratch_shapes=[
            pltpu.VMEM((NX, 2, 128, D), BF16),
            pltpu.VMEM((NZ, NY, 32, 2 * DK), BF16),
            pltpu.VMEM((NZ, NY, 32, DV), BF16),
            pltpu.VMEM((NZ, NY, 32, DV), BF16),
            pltpu.VMEM((1024, DV), F32),
            pltpu.VMEM((1024, DK), BF16),
            pltpu.VMEM((DV, DK), F32),
            pltpu.VMEM((1, DK), F32),
            pltpu.VMEM((64, 8, DK), BF16),
            pltpu.VMEM((1, DK), F32),
            pltpu.VMEM((64, 8, DK), BF16),
            pltpu.VMEM((64, 1, DK), F32),
            pltpu.VMEM((64, 8, DK), BF16),
            pltpu.VMEM((64, 8, DK), BF16),
            pltpu.VMEM((NX, 2, 128, D), BF16),
            pltpu.VMEM((NX, 128, D), BF16),
            pltpu.VMEM((3, 128, D), BF16),
            pltpu.VMEM((64, D), BF16),
            pltpu.VMEM((64, D), BF16),
            pltpu.VMEM((128, D), BF16),
            pltpu.VMEM((128, D), BF16),
            pltpu.SemaphoreType.DMA((14,)),
            pltpu.SemaphoreType.DMA((14,)),
            pltpu.SemaphoreType.DMA((4, 21)),
            pltpu.SemaphoreType.DMA((4, 21)),
            pltpu.SemaphoreType.DMA((3,)),
            pltpu.SemaphoreType.DMA((3,)),
            pltpu.SemaphoreType.DMA((10,)),
            pltpu.SemaphoreType.DMA((10,)),
        ],
        compiler_params=pltpu.CompilerParams(
            collective_id=0, has_side_effects=True, vmem_limit_bytes=56 * 1024 * 1024
        ),
    )(
        tokens,
        norm_gain[None],
        w_query,
        w_key,
        w_value,
        w_rank_down,
        w_rank_up,
        gate_bias[None],
        decay_shift.reshape(NX, QUAD),
        out_gain[None],
        w_out,
    )


def solution(mesh):
    finer = Mesh(mesh.devices.reshape(NZ, NY, NX, 2), ALL)
    in_specs = (
        P(ALL, None),
        P(),
        P(SP, TP),
        P(SP, TP),
        P(SP, TP),
        P(),
        P(None, TP),
        P(TP),
        P(SP),
        P(),
        P(TP, SP),
    )
    return jax.shard_map(on_device, mesh=finer, in_specs=in_specs, out_specs=P(ALL, None), check_vma=False)
```

```python
import jax
import jax.numpy as jnp
from jax import lax
from jax.experimental import pallas as pl
from jax.experimental.pallas import tpu as pltpu
from jax.sharding import Mesh
from jax.sharding import PartitionSpec as P

DK = 256
DV = 512
TAU = 16
BLOCK = 64
QUAD = 256
D = 2048
EPS = 1e-06
NY = NZ = 8
NX = 4
SP = ("z", "y")
TP = ("x", "c")
ALL = ("z", "y", "x", "c")
MESH = pl.DeviceIdType.MESH
VMEM = pl.BlockSpec(memory_space=pltpu.VMEM)
ANY = pl.BlockSpec(memory_space=pl.ANY)
BF16 = jnp.bfloat16
F32 = jnp.float32
NN, NT, TN = (((1,), (0,)), ((1,), (1,)), ((0,), (0,)))


def dot(a, b, dims):
    return lax.dot_general(a, b, (dims, ((), ())), preferred_element_type=F32)


def positions():
    return (lax.broadcasted_iota(jnp.int32, (QUAD, QUAD), i) for i in range(2))


def split3(value):
    hi = value.astype(BF16)
    rest = value - hi.astype(F32)
    mid = rest.astype(BF16)
    low = (rest - mid.astype(F32)).astype(BF16)
    return hi, mid, low


def remote(src, dst, send, recv, **device):
    return pltpu.make_async_remote_copy(
        src_ref=src, dst_ref=dst, send_sem=send, recv_sem=recv, device_id=device, device_id_type=MESH
    )


class Spread:
    def __init__(self, buf, at, rows, first, send, recv):
        self.buf, self.rows, self.send, self.recv = buf, rows, send, recv
        self.first, self.second = first, "z" if first == "y" else "y"
        self.at = at
        self.where = {"y": lax.axis_index("y"), "z": lax.axis_index("z")}

    def rest(self):
        return (pl.ds(self.at, self.rows), slice(None))

    def shard(self, along):
        pos = dict(self.where)
        pos[self.first] = along
        return self.buf.at[(pos["z"], pos["y"]) + self.rest()]

    def half(self, line, h):
        part = pl.ds(4 * h, 4)
        lead = (line, part) if self.second == "z" else (part, line)
        return self.buf.at[lead + self.rest()]

    def push(self, d):
        mine = self.where[self.first]
        ref = self.shard(mine)
        return remote(ref, ref, self.send.at[d - 1], self.recv.at[d - 1], **{self.first: lax.rem(mine + d, 8)})

    def start_push(self):
        for d in (1, 7, 2, 6, 3, 5, 4):
            self.push(d).start()

    def wait_push(self):
        mine = self.where[self.first]
        for d in (1, 7, 2, 6, 3, 5, 4):
            ref = self.shard(lax.rem(mine - d + 8, 8))
            remote(ref, ref, self.send.at[d - 1], self.recv.at[d - 1], **{self.first: mine}).wait_recv()

    def hop(self, s, h, way):
        mine = self.where[self.second]
        step = 1 if way == 0 else 7
        line = lax.rem(mine + (8 - step) * (s - 1), 8)
        ref = self.half(line, h)
        i = 7 + way * 7 + 2 * (s - 1) + (h if s < 4 else 0)
        return remote(ref, ref, self.send.at[i], self.recv.at[i], **{self.second: lax.rem(mine + step, 8)})

    def wait_hop(self, s, h, way):
        mine = self.where[self.second]
        step = 1 if way == 0 else 7
        ref = self.half(lax.rem(mine + (8 - step) * s, 8), h)
        i = 7 + way * 7 + 2 * (s - 1) + (h if s < 4 else 0)
        remote(ref, ref, self.send.at[i], self.recv.at[i], **{self.second: mine}).wait_recv()

    def hops(self, s):
        if s < 4:
            return [(0, 0), (1, 1), (1, 0), (0, 1)]
        return [(0, 0), (1, 1)]

    def finish(self):
        self.wait_hop(3, 1, 0)
        self.wait_hop(3, 0, 1)
        self.wait_hop(4, 0, 0)
        self.wait_hop(4, 1, 1)

    def drain(self):
        for d in range(1, 8):
            self.push(d).wait_send()
        for s in range(1, 5):
            for h, way in self.hops(s):
                self.hop(s, h, way).wait_send()


class FineSpread(Spread):
    def half(self, line, h):
        pair = lax.rem(lax.div(self.where[self.first], 2) + h, 4)
        part = pl.ds(2 * pair, 2)
        lead = (line, part) if self.second == "z" else (part, line)
        return self.buf.at[lead + self.rest()]

    def wait_from(self, d):
        mine = self.where[self.first]
        ref = self.shard(lax.rem(mine - d + 8, 8))
        remote(ref, ref, self.send.at[d - 1], self.recv.at[d - 1], **{self.first: mine}).wait_recv()

    def wait_pair(self, h):
        mine = self.where[self.first]
        odd = lax.rem(mine, 2)
        if h == 0:
            self.wait_from(7 - 6 * odd)
        else:
            for d in range(2):
                self.wait_from(lax.rem(8 - 2 * h + odd - d, 8))

    def index(self, s, h, way):
        return 7 + 14 * way + 4 * (s - 1) + (h if s < 4 else h // 2)

    def hop(self, s, h, way):
        mine = self.where[self.second]
        step = 1 if way == 0 else 7
        ref = self.half(lax.rem(mine + (8 - step) * (s - 1), 8), h)
        i = self.index(s, h, way)
        return remote(ref, ref, self.send.at[i], self.recv.at[i], **{self.second: lax.rem(mine + step, 8)})

    def wait_hop(self, s, h, way):
        mine = self.where[self.second]
        step = 1 if way == 0 else 7
        ref = self.half(lax.rem(mine + (8 - step) * s, 8), h)
        i = self.index(s, h, way)
        remote(ref, ref, self.send.at[i], self.recv.at[i], **{self.second: mine}).wait_recv()

    def hops(self, s):
        both = [(0, 0), (0, 1), (1, 0), (1, 1), (3, 0), (3, 1), (2, 0), (2, 1)]
        return both if s < 4 else [(0, 0), (1, 1), (2, 0), (3, 1)]

    def finish(self):
        for h in range(4):
            self.wait_hop(3, h, 1 - h % 2)
            self.wait_hop(4, h, h % 2)


def relay(pieces, s):
    for k in range(len(pieces[0].hops(s))):
        for p in pieces:
            h, way = p.hops(s)[k]
            if s > 1:
                p.wait_hop(s - 1, h, way)
            elif way == 0 and isinstance(p, FineSpread):
                p.wait_pair(h)
            p.hop(s, h, way).start()


def layer_kernel(
    tok_hbm,
    gain_ref,
    wq_hbm,
    wk_hbm,
    wv_hbm,
    down_ref,
    up_ref,
    bias_ref,
    shift_ref,
    ogain_ref,
    wo_hbm,
    out_ref,
    tok_ref,
    xn,
    wkv,
    wqb,
    wo,
    kv_ref,
    cum_ref,
    base_ref,
    starts,
    att_ref,
    far_ref,
    state_ref,
    give,
    decay_out,
    got,
    decays,
    answer,
    carried,
    part,
    other,
    chip,
    ring_l,
    ring_r,
    from_l,
    from_r,
    in_sem,
    tok_send,
    tok_recv,
    kv_send,
    kv_recv,
    w_send,
    w_recv,
    scan_send,
    scan_recv,
    rs_send,
    rs_recv,
):
    z, y, x, c = (lax.axis_index(a) for a in ALL)
    sp = z * NY + y
    right, left, mate = lax.rem(x + 1, NX), lax.rem(x + NX - 1, NX), 1 - c

    def peer(d):
        p = lax.rem(sp + d, 64)
        return {"z": lax.div(p, 8), "y": lax.rem(p, 8)}

    barrier = pltpu.get_barrier_semaphore()
    near = [{"x": right}, {"x": left}, {"c": mate}]
    near += [{a: lax.rem(i + d, 8)} for a, i in (("y", y), ("z", z)) for d in range(1, 8)]
    for device in near:
        pl.semaphore_signal(barrier, inc=1, device_id=device, device_id_type=MESH)

    loads = (
        pltpu.make_async_copy(wk_hbm, wkv.at[z, y, :, pl.ds(0, DK)], in_sem.at[0]),
        pltpu.make_async_copy(wv_hbm, wkv.at[z, y, :, pl.ds(DK, DV)], in_sem.at[1]),
        pltpu.make_async_copy(tok_hbm.at[pl.ds(0, 64)], tok_ref.at[pl.ds(0, 64)], in_sem.at[2]),
        pltpu.make_async_copy(tok_hbm.at[pl.ds(64, 64)], tok_ref.at[pl.ds(64, 64)], in_sem.at[3]),
        pltpu.make_async_copy(wq_hbm, wqb.at[z, y], in_sem.at[4]),
        pltpu.make_async_copy(wo_hbm, wo.at[z, y], in_sem.at[5]),
    )
    for load in loads:
        load.start()

    kv = tuple(FineSpread(wkv, 16 * i, 16, "yz"[i], kv_send.at[i], kv_recv.at[i]) for i in range(2))
    qs = tuple(Spread(wqb, 16 * i, 16, "yz"[i], w_send.at[i], w_recv.at[i]) for i in range(2))
    outs = tuple(Spread(wo, 16 * i, 16, "yz"[i], w_send.at[2 + i], w_recv.at[2 + i]) for i in range(2))

    def start_push(pieces):
        for p in pieces:
            p.start_push()

    def wait_push(pieces):
        for p in pieces:
            p.wait_push()

    def rows_of(xx, h):
        return xn.at[xx, c, pl.ds(64 * h, 64), :]

    def token(i, xx, h, to):
        ref = rows_of(xx, h)
        return remote(ref, ref, tok_send.at[i], tok_recv.at[i], x=to)

    def to_mate(i, xx, h):
        ref = rows_of(xx, h)
        return remote(ref, ref, tok_send.at[i], tok_recv.at[i], c=mate)

    def norm(h):
        rows = slice(64 * h, 64 * h + 64)
        wide = tok_ref[rows, :].astype(F32)
        normed = wide * lax.rsqrt(jnp.mean(wide * wide, axis=-1, keepdims=True) + EPS) * gain_ref[...]
        xn[x, c, rows, :] = normed.astype(BF16)

    far_x = lax.rem(x + 2, NX)
    sends = []

    def go(copy):
        copy.start()
        sends.append(copy)

    def arrive(i, xx, h, slot):
        token(i, xx, h, x).wait_recv()
        go(to_mate(slot, xx, h))

    def from_mate(i, xx, h):
        ref = xn.at[xx, mate, pl.ds(64 * h, 64), :]
        remote(ref, ref, tok_send.at[i], tok_recv.at[i], c=mate).wait_recv()

    row, col = positions()
    lower = jnp.where(col <= row, 1.0, 0.0).astype(BF16)

    def gates(i):
        rank = dot(xn[i].reshape(QUAD, D), down_ref[...], NT).astype(BF16)
        pre = dot(rank, up_ref[...], NN) + bias_ref[...]
        logs = jnp.minimum(pre, 0.0) - jnp.log1p(jnp.exp(-jnp.abs(pre)))
        ones = jnp.ones((8, DK), BF16)
        shift = shift_ref[:, pl.ds(pl.multiple_of(i * QUAD, QUAD), QUAD)]
        shifts = sum(dot(jnp.broadcast_to(t.astype(F32), (8, QUAD)).astype(BF16), ones, TN) for t in split3(shift)) * 0.125
        hi, mid, low = split3(logs * (1.0 / TAU) + shifts)
        cum_ref[i] = dot(lower, hi, NN) + (dot(lower, mid, NN) + dot(lower, low, NN))

    loads[0].wait()
    loads[1].wait()
    pl.semaphore_wait(barrier, 17)
    start_push(kv)
    loads[2].wait()
    norm(0)
    go(token(0, x, 0, right))
    go(to_mate(6, x, 0))
    loads[3].wait()
    norm(1)
    go(token(3, x, 1, left))
    go(to_mate(7, x, 1))
    go(token(1, x, 1, right))
    go(token(4, x, 0, left))
    relay(kv, 1)
    from_mate(6, x, 0)
    from_mate(7, x, 1)
    gates(x)
    arrive(0, left, 0, 8)
    go(token(2, left, 0, right))
    arrive(3, right, 1, 9)
    go(token(5, right, 1, left))
    relay(kv, 2)
    relay(kv, 3)
    arrive(1, left, 1, 10)
    arrive(4, right, 0, 11)
    relay(kv, 4)
    loads[4].wait()
    start_push(qs)
    loads[5].wait()
    start_push(outs)
    from_mate(8, left, 0)
    from_mate(10, left, 1)
    gates(left)
    from_mate(9, right, 1)
    from_mate(11, right, 0)
    gates(right)
    arrive(2, far_x, 0, 12)
    arrive(5, far_x, 1, 13)
    from_mate(12, far_x, 0)
    from_mate(13, far_x, 1)
    gates(far_x)
    base = jnp.zeros((1, DK), F32)
    for i in range(NX):
        base_ref[i] = base
        base = base + cum_ref[i, QUAD - 1 : QUAD]
    decay_out[...] = jnp.exp(base)
    for p in kv:
        p.finish()

    state_ref[...] = jnp.zeros_like(state_ref)

    def absorb(i, carry):
        @pl.when(i == 1)
        def _():
            wait_push(qs)
            relay(qs, 1)

        @pl.when(i == 3)
        def _():
            relay(qs, 2)

        now = dot(xn[i].reshape(QUAD, D), wkv[...].reshape(D, DK + DV), NN).astype(BF16)
        kv_ref[pl.ds(pl.multiple_of(i * QUAD, QUAD), QUAD), :] = now
        cum = cum_ref[i]
        final = cum[QUAD - 1 : QUAD]
        decayed = (now[:, 0:DK].astype(F32) * jnp.exp(final - cum)).astype(BF16)
        state = state_ref[...]
        starts[i] = state.astype(BF16)
        state_ref[...] = jnp.exp(final) * state + dot(now[:, DK:], decayed, TN)
        return carry

    lax.fori_loop(0, NX, absorb, 0)

    give[...] = state_ref[...].reshape(64, 8, DK).astype(BF16)

    def ask(d):
        p = peer(d)
        j = p["z"] * NY + p["y"]
        return (
            remote(give.at[j], got.at[sp], scan_send.at[0], scan_recv.at[0], **p),
            remote(decay_out, decays.at[sp], scan_send.at[1], scan_recv.at[1], **p),
        )

    def reply(d):
        p = peer(d)
        j = p["z"] * NY + p["y"]
        return remote(answer.at[j], carried.at[sp], scan_send.at[2], scan_recv.at[2], **p)

    def start_ask(d, carry):
        for r in ask(d):
            r.start()
        return carry

    def start_reply(d, carry):
        reply(d).start()
        return carry

    def wait_all(ref, sem):
        most = ref.at[pl.ds(0, 63)]
        pltpu.make_async_copy(most, most, sem).wait()

    lax.fori_loop(1, 64, start_ask, 0)
    got[sp] = give[sp]
    decays[sp] = decay_out[...]
    relay(qs, 3)
    wait_push(outs)
    relay(outs, 1)
    relay(qs, 4)
    relay(outs, 2)
    for p in qs:
        p.finish()
    relay(outs, 3)

    def attend(i, carry):
        at = pl.ds(pl.multiple_of(i * QUAD, QUAD), QUAD)
        q = dot(xn[i].reshape(QUAD, D), wqb[...].reshape(D, DK), NN).astype(BF16).astype(F32) * DK ** (-0.5)
        k = kv_ref[at, 0:DK].astype(F32)
        v = kv_ref[at, DK : DK + DV]
        cum = cum_ref[i]
        cube = cum.reshape(QUAD // BLOCK, BLOCK, DK)
        centre = (cube - cube[:, BLOCK // 2 : BLOCK // 2 + 1]).reshape(QUAD, DK)
        q_scaled = (q * jnp.exp(centre)).astype(BF16)
        k_scaled = (k * jnp.exp(-centre)).astype(BF16)
        causal = (row // BLOCK == col // BLOCK) & (col <= row)
        scores = jnp.where(causal, dot(q_scaled, k_scaled, NT), 0.0)
        lines = [scores[0:BLOCK]]
        for n in range(1, QUAD // BLOCK):
            cut = n * BLOCK
            edge = cum[cut - 1 : cut]
            q_part = (q[cut : cut + BLOCK] * jnp.exp(cum[cut : cut + BLOCK] - edge)).astype(BF16)
            k_part = (k[0:cut] * jnp.exp(edge - cum[0:cut])).astype(BF16)
            k_part = jnp.concatenate([k_part, jnp.zeros((QUAD - cut, DK), BF16)], axis=0)
            lines.append(scores[cut : cut + BLOCK] + dot(q_part, k_part, NT))
        scores = jnp.concatenate(lines, axis=0).astype(BF16)
        reach = q * jnp.exp(cum)
        att_ref[at, :] = dot(scores, v, NN) + dot(reach.astype(BF16), starts[i], NT)
        far_ref[at, :] = (reach * jnp.exp(base_ref[i])).astype(BF16)
        return carry

    wait_all(got, scan_recv.at[0])
    wait_all(decays, scan_recv.at[1])

    def prefix(j, carry):
        answer[j] = carry.astype(BF16)
        return decays[j] * carry + got[j].astype(F32)

    lax.fori_loop(0, 64, prefix, jnp.zeros((8, DK), F32))
    lax.fori_loop(1, 64, start_reply, 0)
    relay(outs, 4)
    lax.fori_loop(0, NX, attend, 0)
    carried[sp] = answer[sp]
    for p in outs:
        p.finish()
    wait_all(carried, scan_recv.at[2])

    halves = (pl.ds(0, 64), pl.ds(64, 64))

    def swap(k):
        return remote(part.at[k, mate], other.at[k], rs_send.at[k], rs_recv.at[k], c=mate)

    def ring(i, src, dst, to):
        return remote(src, dst, rs_send.at[4 + i], rs_recv.at[4 + i], x=to)

    hops = (
        ring(0, chip.at[0, halves[0]], ring_l, right),
        ring(1, chip.at[0, halves[1]], ring_r, left),
        ring(2, chip.at[1, halves[1]], from_l.at[halves[1]], right),
        ring(3, chip.at[2, halves[0]], from_r.at[halves[0]], left),
        ring(4, chip.at[1, halves[0]], from_l.at[halves[0]], right),
        ring(5, chip.at[2, halves[1]], from_r.at[halves[1]], left),
    )

    def both(k, rows):
        return part[k, c, rows, :].astype(F32) + other[k, rows, :].astype(F32)

    def finish(k, carry):
        off = jnp.where(k == 0, 2, jnp.where(k == 1, 1, jnp.where(k == 2, 3, 0)))
        to = lax.rem(x + off, NX)
        at = pl.ds(pl.multiple_of(to * QUAD, QUAD), QUAD)
        att = att_ref[at, :] + dot(far_ref[at, :], carried[...].reshape(DV, DK), NT)
        shaped = att * lax.rsqrt(jnp.mean(att * att, axis=-1, keepdims=True) + EPS) * ogain_ref[...]
        res = dot(shaped.astype(BF16), wo[...].reshape(D, DV), NT).astype(BF16)
        part[k] = res.reshape(2, 128, D)
        swap(k).start()

        @pl.when(k == 1)
        def _():
            swap(0).wait_recv()
            chip[0] = both(0, slice(None)).astype(BF16)
            hops[0].start()
            hops[1].start()

        @pl.when(k == 2)
        def _():
            swap(1).wait_recv()
            chip[1, halves[1], :] = both(1, halves[1]).astype(BF16)
            hops[2].start()

        @pl.when(k == 3)
        def _():
            swap(2).wait_recv()
            chip[2, halves[0], :] = both(2, halves[0]).astype(BF16)
            hops[3].start()

        return carry

    lax.fori_loop(0, NX, finish, 0)
    hops[0].wait_recv()
    chip[1, halves[0], :] = (both(1, halves[0]) + ring_l[...].astype(F32)).astype(BF16)
    hops[4].start()
    hops[1].wait_recv()
    chip[2, halves[1], :] = (both(2, halves[1]) + ring_r[...].astype(F32)).astype(BF16)
    hops[5].start()
    swap(3).wait_recv()
    for i in (2, 3, 4, 5):
        hops[i].wait_recv()
    out_ref[...] = (both(3, slice(None)) + from_l[...].astype(F32) + from_r[...].astype(F32)).astype(BF16)

    for s in sends:
        s.wait_send()
    for p in kv + qs + outs:
        p.drain()
    sent = give.at[pl.ds(0, 63)]
    pltpu.make_async_copy(sent, sent, scan_send.at[0]).wait()
    wait_all(decays, scan_send.at[1])
    wait_all(answer, scan_send.at[2])
    for k in range(4):
        swap(k).wait_send()
    for h in hops:
        h.wait_send()


def on_device(
    tokens,
    norm_gain,
    w_query,
    w_key,
    w_value,
    w_rank_down,
    w_rank_up,
    gate_bias,
    decay_shift,
    out_gain,
    w_out,
):
    return pl.pallas_call(
        layer_kernel,
        out_shape=jax.ShapeDtypeStruct(tokens.shape, BF16),
        in_specs=[ANY, VMEM, ANY, ANY, ANY, VMEM, VMEM, VMEM, VMEM, VMEM, ANY],
        out_specs=VMEM,
        scratch_shapes=[
            pltpu.VMEM((128, D), BF16),
            pltpu.VMEM((NX, 2, 128, D), BF16),
            pltpu.VMEM((NZ, NY, 32, DK + DV), BF16),
            pltpu.VMEM((NZ, NY, 32, DK), BF16),
            pltpu.VMEM((NZ, NY, 32, DV), BF16),
            pltpu.VMEM((NX * QUAD, DK + DV), BF16),
            pltpu.VMEM((NX, QUAD, DK), F32),
            pltpu.VMEM((NX, 1, DK), F32),
            pltpu.VMEM((NX, DV, DK), BF16),
            pltpu.VMEM((NX * QUAD, DV), F32),
            pltpu.VMEM((NX * QUAD, DK), BF16),
            pltpu.VMEM((DV, DK), F32),
            pltpu.VMEM((64, 8, DK), BF16),
            pltpu.VMEM((1, DK), F32),
            pltpu.VMEM((64, 8, DK), BF16),
            pltpu.VMEM((64, 1, DK), F32),
            pltpu.VMEM((64, 8, DK), BF16),
            pltpu.VMEM((64, 8, DK), BF16),
            pltpu.VMEM((NX, 2, 128, D), BF16),
            pltpu.VMEM((NX, 128, D), BF16),
            pltpu.VMEM((3, 128, D), BF16),
            pltpu.VMEM((64, D), BF16),
            pltpu.VMEM((64, D), BF16),
            pltpu.VMEM((128, D), BF16),
            pltpu.VMEM((128, D), BF16),
            pltpu.SemaphoreType.DMA((6,)),
            pltpu.SemaphoreType.DMA((14,)),
            pltpu.SemaphoreType.DMA((14,)),
            pltpu.SemaphoreType.DMA((2, 35)),
            pltpu.SemaphoreType.DMA((2, 35)),
            pltpu.SemaphoreType.DMA((4, 21)),
            pltpu.SemaphoreType.DMA((4, 21)),
            pltpu.SemaphoreType.DMA((3,)),
            pltpu.SemaphoreType.DMA((3,)),
            pltpu.SemaphoreType.DMA((10,)),
            pltpu.SemaphoreType.DMA((10,)),
        ],
        compiler_params=pltpu.CompilerParams(
            collective_id=0, has_side_effects=True, vmem_limit_bytes=56 * 1024 * 1024
        ),
    )(
        tokens,
        norm_gain[None],
        w_query,
        w_key,
        w_value,
        w_rank_down.T,
        w_rank_up,
        gate_bias[None],
        decay_shift[None],
        out_gain[None],
        w_out.T,
    )


def solution(mesh):
    finer = Mesh(mesh.devices.reshape(NZ, NY, NX, 2), ALL)
    in_specs = (
        P(ALL, None),
        P(),
        P(SP, TP),
        P(SP, TP),
        P(SP, TP),
        P(),
        P(None, TP),
        P(TP),
        P(SP),
        P(),
        P(TP, SP),
    )
    return jax.shard_map(on_device, mesh=finer, in_specs=in_specs, out_specs=P(ALL, None), check_vma=False)
```

```python
import jax
import jax.numpy as jnp
from jax import lax
from jax.experimental import pallas as pl
from jax.experimental.pallas import tpu as pltpu
from jax.sharding import Mesh
from jax.sharding import PartitionSpec as P

DK = 256
DV = 512
TAU = 16
BLOCK = 64
QUAD = 256
D = 2048
EPS = 1e-06
NY = NZ = 8
NX = 4
SP = ("z", "y")
TP = ("x", "c")
ALL = ("z", "y", "x", "c")
MESH = pl.DeviceIdType.MESH
VMEM = pl.BlockSpec(memory_space=pltpu.VMEM)
HBM = pl.BlockSpec(memory_space=pltpu.HBM)
BF16 = jnp.bfloat16
F32 = jnp.float32
NN, NT, TN = (((1,), (0,)), ((1,), (1,)), ((0,), (0,)))


def dot(a, b, dims):
    return lax.dot_general(a, b, (dims, ((), ())), preferred_element_type=F32)


def positions():
    return (lax.broadcasted_iota(jnp.int32, (QUAD, QUAD), i) for i in range(2))


def split3(value):
    hi = value.astype(BF16)
    rest = value - hi.astype(F32)
    mid = rest.astype(BF16)
    low = (rest - mid.astype(F32)).astype(BF16)
    return hi, mid, low


def remote(src, dst, send, recv, **device):
    return pltpu.make_async_remote_copy(
        src_ref=src, dst_ref=dst, send_sem=send, recv_sem=recv, device_id=device, device_id_type=MESH
    )


class Spread:
    def __init__(self, buf, at, rows, first, send, recv):
        self.buf, self.rows, self.send, self.recv = buf, rows, send, recv
        self.first, self.second = first, "z" if first == "y" else "y"
        self.at = at
        self.where = {"y": lax.axis_index("y"), "z": lax.axis_index("z")}

    def rest(self):
        return (pl.ds(self.at, self.rows), slice(None))

    def shard(self, along):
        pos = dict(self.where)
        pos[self.first] = along
        return self.buf.at[(pos["z"], pos["y"]) + self.rest()]

    def half(self, line, h):
        part = pl.ds(4 * h, 4)
        lead = (line, part) if self.second == "z" else (part, line)
        return self.buf.at[lead + self.rest()]

    def push(self, d):
        mine = self.where[self.first]
        ref = self.shard(mine)
        return remote(ref, ref, self.send.at[d - 1], self.recv.at[d - 1], **{self.first: lax.rem(mine + d, 8)})

    def start_push(self):
        for d in (1, 7, 2, 6, 3, 5, 4):
            self.push(d).start()

    def wait_push(self):
        mine = self.where[self.first]
        for d in (1, 7, 2, 6, 3, 5, 4):
            ref = self.shard(lax.rem(mine - d + 8, 8))
            remote(ref, ref, self.send.at[d - 1], self.recv.at[d - 1], **{self.first: mine}).wait_recv()

    def hop(self, s, h, way):
        mine = self.where[self.second]
        step = 1 if way == 0 else 7
        line = lax.rem(mine + (8 - step) * (s - 1), 8)
        ref = self.half(line, h)
        i = 7 + way * 7 + 2 * (s - 1) + (h if s < 4 else 0)
        return remote(ref, ref, self.send.at[i], self.recv.at[i], **{self.second: lax.rem(mine + step, 8)})

    def wait_hop(self, s, h, way):
        mine = self.where[self.second]
        step = 1 if way == 0 else 7
        ref = self.half(lax.rem(mine + (8 - step) * s, 8), h)
        i = 7 + way * 7 + 2 * (s - 1) + (h if s < 4 else 0)
        remote(ref, ref, self.send.at[i], self.recv.at[i], **{self.second: mine}).wait_recv()

    def hops(self, s):
        if s < 4:
            return [(0, 0), (1, 1), (1, 0), (0, 1)]
        return [(0, 0), (1, 1)]

    def finish(self):
        self.wait_hop(3, 1, 0)
        self.wait_hop(3, 0, 1)
        self.wait_hop(4, 0, 0)
        self.wait_hop(4, 1, 1)

    def drain(self):
        for d in range(1, 8):
            self.push(d).wait_send()
        for s in range(1, 5):
            for h, way in self.hops(s):
                self.hop(s, h, way).wait_send()


class FineSpread(Spread):
    def half(self, line, h):
        pair = lax.rem(lax.div(self.where[self.first], 2) + h, 4)
        part = pl.ds(2 * pair, 2)
        lead = (line, part) if self.second == "z" else (part, line)
        return self.buf.at[lead + self.rest()]

    def wait_from(self, d):
        mine = self.where[self.first]
        ref = self.shard(lax.rem(mine - d + 8, 8))
        remote(ref, ref, self.send.at[d - 1], self.recv.at[d - 1], **{self.first: mine}).wait_recv()

    def wait_pair(self, h):
        mine = self.where[self.first]
        odd = lax.rem(mine, 2)
        if h == 0:
            self.wait_from(7 - 6 * odd)
        else:
            for d in range(2):
                self.wait_from(lax.rem(8 - 2 * h + odd - d, 8))

    def index(self, s, h, way):
        return 7 + 14 * way + 4 * (s - 1) + (h if s < 4 else h // 2)

    def hop(self, s, h, way):
        mine = self.where[self.second]
        step = 1 if way == 0 else 7
        ref = self.half(lax.rem(mine + (8 - step) * (s - 1), 8), h)
        i = self.index(s, h, way)
        return remote(ref, ref, self.send.at[i], self.recv.at[i], **{self.second: lax.rem(mine + step, 8)})

    def wait_hop(self, s, h, way):
        mine = self.where[self.second]
        step = 1 if way == 0 else 7
        ref = self.half(lax.rem(mine + (8 - step) * s, 8), h)
        i = self.index(s, h, way)
        remote(ref, ref, self.send.at[i], self.recv.at[i], **{self.second: mine}).wait_recv()

    def hops(self, s):
        both = [(0, 0), (0, 1), (1, 0), (1, 1), (3, 0), (3, 1), (2, 0), (2, 1)]
        return both if s < 4 else [(0, 0), (1, 1), (2, 0), (3, 1)]

    def finish(self):
        for h in range(4):
            self.wait_hop(3, h, 1 - h % 2)
            self.wait_hop(4, h, h % 2)


def relay(pieces, s):
    for k in range(len(pieces[0].hops(s))):
        for p in pieces:
            h, way = p.hops(s)[k]
            if s > 1:
                p.wait_hop(s - 1, h, way)
            elif way == 0 and isinstance(p, FineSpread):
                p.wait_pair(h)
            p.hop(s, h, way).start()


def layer_kernel(
    tok_hbm,
    gain_hbm,
    wq_hbm,
    wk_hbm,
    wv_hbm,
    down_hbm,
    up_hbm,
    bias_hbm,
    shift_hbm,
    ogain_hbm,
    wo_hbm,
    own_ref,
    from_l,
    from_r,
    tok_ref,
    xn,
    wkv,
    wqb,
    wo,
    kv_ref,
    cum_ref,
    base_ref,
    starts,
    att_ref,
    far_ref,
    state_ref,
    give,
    decay_out,
    got,
    decays,
    answer,
    carried,
    part,
    other,
    chip,
    ring_l,
    ring_r,
    gain_ref,
    down_ref,
    up_ref,
    bias_ref,
    shift_ref,
    ogain_ref,
    in_sem,
    tok_send,
    tok_recv,
    kv_send,
    kv_recv,
    w_send,
    w_recv,
    scan_send,
    scan_recv,
    rs_send,
    rs_recv,
):
    z, y, x, c = (lax.axis_index(a) for a in ALL)
    sp = z * NY + y
    right, left, mate = lax.rem(x + 1, NX), lax.rem(x + NX - 1, NX), 1 - c

    def peer(d):
        p = lax.rem(sp + d, 64)
        return {"z": lax.div(p, 8), "y": lax.rem(p, 8)}

    barrier = pltpu.get_barrier_semaphore()
    near = [{"x": right}, {"x": left}, {"c": mate}]
    near += [{a: lax.rem(i + d, 8)} for a, i in (("y", y), ("z", z)) for d in range(1, 8)]
    for device in near:
        pl.semaphore_signal(barrier, inc=1, device_id=device, device_id_type=MESH)

    loads = (
        pltpu.make_async_copy(wk_hbm, wkv.at[z, y, :, pl.ds(0, DK)], in_sem.at[0]),
        pltpu.make_async_copy(wv_hbm, wkv.at[z, y, :, pl.ds(DK, DV)], in_sem.at[1]),
        pltpu.make_async_copy(tok_hbm.at[pl.ds(0, 64)], tok_ref.at[pl.ds(0, 64)], in_sem.at[2]),
        pltpu.make_async_copy(tok_hbm.at[pl.ds(64, 64)], tok_ref.at[pl.ds(64, 64)], in_sem.at[3]),
        pltpu.make_async_copy(wq_hbm, wqb.at[z, y], in_sem.at[4]),
        pltpu.make_async_copy(wo_hbm, wo.at[z, y], in_sem.at[5]),
        pltpu.make_async_copy(gain_hbm, gain_ref, in_sem.at[6]),
        pltpu.make_async_copy(down_hbm, down_ref, in_sem.at[7]),
        pltpu.make_async_copy(up_hbm, up_ref, in_sem.at[8]),
        pltpu.make_async_copy(bias_hbm, bias_ref, in_sem.at[9]),
        pltpu.make_async_copy(shift_hbm, shift_ref, in_sem.at[10]),
        pltpu.make_async_copy(ogain_hbm, ogain_ref, in_sem.at[11]),
    )
    for load in loads:
        load.start()

    kv = tuple(FineSpread(wkv, 16 * i, 16, "yz"[i], kv_send.at[i], kv_recv.at[i]) for i in range(2))
    qs = tuple(Spread(wqb, 16 * i, 16, "yz"[i], w_send.at[i], w_recv.at[i]) for i in range(2))
    outs = tuple(Spread(wo, 16 * i, 16, "yz"[i], w_send.at[2 + i], w_recv.at[2 + i]) for i in range(2))

    def start_push(pieces):
        for p in pieces:
            p.start_push()

    def wait_push(pieces):
        for p in pieces:
            p.wait_push()

    def rows_of(xx, h):
        return xn.at[xx, c, pl.ds(64 * h, 64), :]

    def token(i, xx, h, to):
        ref = rows_of(xx, h)
        return remote(ref, ref, tok_send.at[i], tok_recv.at[i], x=to)

    def to_mate(i, xx, h):
        ref = rows_of(xx, h)
        return remote(ref, ref, tok_send.at[i], tok_recv.at[i], c=mate)

    def norm(h):
        rows = slice(64 * h, 64 * h + 64)
        wide = tok_ref[rows, :].astype(F32)
        normed = wide * lax.rsqrt(jnp.mean(wide * wide, axis=-1, keepdims=True) + EPS) * gain_ref[...]
        xn[x, c, rows, :] = normed.astype(BF16)

    far_x = lax.rem(x + 2, NX)
    sends = []

    def go(copy):
        copy.start()
        sends.append(copy)

    def arrive(i, xx, h, slot):
        token(i, xx, h, x).wait_recv()
        go(to_mate(slot, xx, h))

    def from_mate(i, xx, h):
        ref = xn.at[xx, mate, pl.ds(64 * h, 64), :]
        remote(ref, ref, tok_send.at[i], tok_recv.at[i], c=mate).wait_recv()

    row, col = positions()
    lower = jnp.where(col <= row, 1.0, 0.0).astype(BF16)

    def gates(i):
        rank = dot(xn[i].reshape(QUAD, D), down_ref[...], NT).astype(BF16)
        pre = dot(rank, up_ref[...], NN) + bias_ref[...]
        logs = jnp.minimum(pre, 0.0) - jnp.log1p(jnp.exp(-jnp.abs(pre)))
        ones = jnp.ones((8, DK), BF16)
        shift = shift_ref[:, pl.ds(pl.multiple_of(i * QUAD, QUAD), QUAD)]
        shifts = sum(dot(jnp.broadcast_to(t.astype(F32), (8, QUAD)).astype(BF16), ones, TN) for t in split3(shift)) * 0.125
        hi, mid, low = split3(logs * (1.0 / TAU) + shifts)
        cum_ref[i] = dot(lower, hi, NN) + (dot(lower, mid, NN) + dot(lower, low, NN))

    loads[0].wait()
    loads[1].wait()
    pl.semaphore_wait(barrier, 17)
    start_push(kv)
    loads[2].wait()
    loads[6].wait()
    norm(0)
    go(token(0, x, 0, right))
    go(to_mate(6, x, 0))
    loads[3].wait()
    norm(1)
    go(token(3, x, 1, left))
    go(to_mate(7, x, 1))
    go(token(1, x, 1, right))
    go(token(4, x, 0, left))
    relay(kv, 1)
    from_mate(6, x, 0)
    from_mate(7, x, 1)
    for load in loads[7:]:
        load.wait()
    gates(x)
    relay(kv, 2)
    arrive(0, left, 0, 8)
    go(token(2, left, 0, right))
    arrive(3, right, 1, 9)
    go(token(5, right, 1, left))
    relay(kv, 3)
    arrive(1, left, 1, 10)
    arrive(4, right, 0, 11)
    loads[4].wait()
    start_push(qs)
    relay(kv, 4)
    loads[5].wait()
    start_push(outs)
    wait_push(qs)
    relay(qs, 1)
    from_mate(8, left, 0)
    from_mate(10, left, 1)
    gates(left)
    from_mate(9, right, 1)
    from_mate(11, right, 0)
    gates(right)
    arrive(2, far_x, 0, 12)
    arrive(5, far_x, 1, 13)
    relay(qs, 2)
    from_mate(12, far_x, 0)
    from_mate(13, far_x, 1)
    gates(far_x)
    base = jnp.zeros((1, DK), F32)
    for i in range(NX):
        base_ref[i] = base
        base = base + cum_ref[i, QUAD - 1 : QUAD]
    decay_out[...] = jnp.exp(base)
    for p in kv:
        p.finish()

    state_ref[...] = jnp.zeros_like(state_ref)

    def absorb(i, carry):
        @pl.when(i == 0)
        def _():
            relay(qs, 3)
            wait_push(outs)
            relay(outs, 1)

        @pl.when(i == 2)
        def _():
            relay(qs, 4)

        now = dot(xn[i].reshape(QUAD, D), wkv[...].reshape(D, DK + DV), NN).astype(BF16)
        kv_ref[pl.ds(pl.multiple_of(i * QUAD, QUAD), QUAD), :] = now
        cum = cum_ref[i]
        final = cum[QUAD - 1 : QUAD]
        decayed = (now[:, 0:DK].astype(F32) * jnp.exp(final - cum)).astype(BF16)
        state = state_ref[...]
        starts[i] = state.astype(BF16)
        state_ref[...] = jnp.exp(final) * state + dot(now[:, DK:], decayed, TN)
        return carry

    lax.fori_loop(0, NX, absorb, 0)

    give[...] = state_ref[...].reshape(64, 8, DK).astype(BF16)

    def ask(d):
        p = peer(d)
        j = p["z"] * NY + p["y"]
        return (
            remote(give.at[j], got.at[sp], scan_send.at[0], scan_recv.at[0], **p),
            remote(decay_out, decays.at[sp], scan_send.at[1], scan_recv.at[1], **p),
        )

    def reply(d):
        p = peer(d)
        j = p["z"] * NY + p["y"]
        return remote(answer.at[j], carried.at[sp], scan_send.at[2], scan_recv.at[2], **p)

    def start_ask(d, carry):
        for r in ask(d):
            r.start()
        return carry

    def start_reply(d, carry):
        reply(d).start()
        return carry

    def wait_all(ref, sem):
        most = ref.at[pl.ds(0, 63)]
        pltpu.make_async_copy(most, most, sem).wait()

    relay(outs, 2)
    lax.fori_loop(1, 64, start_ask, 0)
    got[sp] = give[sp]
    decays[sp] = decay_out[...]

    def attend(i, carry):
        at = pl.ds(pl.multiple_of(i * QUAD, QUAD), QUAD)
        q = dot(xn[i].reshape(QUAD, D), wqb[...].reshape(D, DK), NN).astype(BF16).astype(F32) * DK ** (-0.5)
        k = kv_ref[at, 0:DK].astype(F32)
        v = kv_ref[at, DK : DK + DV]
        cum = cum_ref[i]
        cube = cum.reshape(QUAD // BLOCK, BLOCK, DK)
        centre = (cube - cube[:, BLOCK // 2 : BLOCK // 2 + 1]).reshape(QUAD, DK)
        q_scaled = (q * jnp.exp(centre)).astype(BF16)
        k_scaled = (k * jnp.exp(-centre)).astype(BF16)
        causal = (row // BLOCK == col // BLOCK) & (col <= row)
        scores = jnp.where(causal, dot(q_scaled, k_scaled, NT), 0.0)
        lines = [scores[0:BLOCK]]
        for n in range(1, QUAD // BLOCK):
            cut = n * BLOCK
            edge = cum[cut - 1 : cut]
            q_part = (q[cut : cut + BLOCK] * jnp.exp(cum[cut : cut + BLOCK] - edge)).astype(BF16)
            k_part = (k[0:cut] * jnp.exp(edge - cum[0:cut])).astype(BF16)
            k_part = jnp.concatenate([k_part, jnp.zeros((QUAD - cut, DK), BF16)], axis=0)
            lines.append(scores[cut : cut + BLOCK] + dot(q_part, k_part, NT))
        scores = jnp.concatenate(lines, axis=0).astype(BF16)
        reach = q * jnp.exp(cum)
        att_ref[at, :] = dot(scores, v, NN) + dot(reach.astype(BF16), starts[i], NT)
        far_ref[at, :] = (reach * jnp.exp(base_ref[i])).astype(BF16)
        return carry

    for p in qs:
        p.finish()
    lax.fori_loop(0, NX, attend, 0)
    relay(outs, 3)
    wait_all(got, scan_recv.at[0])
    wait_all(decays, scan_recv.at[1])

    def prefix(j, carry):
        answer[j] = carry.astype(BF16)
        return decays[j] * carry + got[j].astype(F32)

    lax.fori_loop(0, 64, prefix, jnp.zeros((8, DK), F32))
    lax.fori_loop(1, 64, start_reply, 0)
    relay(outs, 4)
    for p in outs:
        p.finish()
    carried[sp] = answer[sp]
    wait_all(carried, scan_recv.at[2])

    halves = (pl.ds(0, 64), pl.ds(64, 64))

    def swap(k):
        return remote(part.at[k, mate], other.at[k], rs_send.at[k], rs_recv.at[k], c=mate)

    def ring(i, src, dst, to):
        return remote(src, dst, rs_send.at[4 + i], rs_recv.at[4 + i], x=to)

    hops = (
        ring(0, chip.at[0, halves[0]], ring_l, right),
        ring(1, chip.at[0, halves[1]], ring_r, left),
        ring(2, chip.at[1, halves[1]], from_l.at[halves[1]], right),
        ring(3, chip.at[2, halves[0]], from_r.at[halves[0]], left),
        ring(4, chip.at[1, halves[0]], from_l.at[halves[0]], right),
        ring(5, chip.at[2, halves[1]], from_r.at[halves[1]], left),
    )

    def both(k, rows):
        return part[k, c, rows, :].astype(F32) + other[k, rows, :].astype(F32)

    def finish(k, carry):
        off = jnp.where(k == 0, 2, jnp.where(k == 1, 1, jnp.where(k == 2, 3, 0)))
        to = lax.rem(x + off, NX)
        at = pl.ds(pl.multiple_of(to * QUAD, QUAD), QUAD)
        att = att_ref[at, :] + dot(far_ref[at, :], carried[...].reshape(DV, DK), NT)
        shaped = att * lax.rsqrt(jnp.mean(att * att, axis=-1, keepdims=True) + EPS) * ogain_ref[...]
        res = dot(shaped.astype(BF16), wo[...].reshape(D, DV), NT).astype(BF16)
        part[k] = res.reshape(2, 128, D)
        swap(k).start()

        @pl.when(k == 1)
        def _():
            swap(0).wait_recv()
            chip[0] = both(0, slice(None)).astype(BF16)
            hops[0].start()
            hops[1].start()

        @pl.when(k == 2)
        def _():
            swap(1).wait_recv()
            chip[1, halves[1], :] = both(1, halves[1]).astype(BF16)
            hops[2].start()

        @pl.when(k == 3)
        def _():
            swap(2).wait_recv()
            chip[2, halves[0], :] = both(2, halves[0]).astype(BF16)
            hops[3].start()

        return carry

    lax.fori_loop(0, NX, finish, 0)
    hops[0].wait_recv()
    chip[1, halves[0], :] = (both(1, halves[0]) + ring_l[...].astype(F32)).astype(BF16)
    hops[4].start()
    hops[1].wait_recv()
    chip[2, halves[1], :] = (both(2, halves[1]) + ring_r[...].astype(F32)).astype(BF16)
    hops[5].start()
    swap(3).wait_recv()
    for i in (2, 3, 4, 5):
        hops[i].wait_recv()
    own_ref[...] = both(3, slice(None))

    for s in sends:
        s.wait_send()
    for p in kv + qs + outs:
        p.drain()
    sent = give.at[pl.ds(0, 63)]
    pltpu.make_async_copy(sent, sent, scan_send.at[0]).wait()
    wait_all(decays, scan_send.at[1])
    wait_all(answer, scan_send.at[2])
    for k in range(4):
        swap(k).wait_send()
    for h in hops:
        h.wait_send()


def on_device(
    tokens,
    norm_gain,
    w_query,
    w_key,
    w_value,
    w_rank_down,
    w_rank_up,
    gate_bias,
    decay_shift,
    out_gain,
    w_out,
):
    inputs = [
        pltpu.with_memory_space_constraint(a, pltpu.HBM)
        for a in (
            tokens,
            norm_gain[None],
            w_query,
            w_key,
            w_value,
            w_rank_down.T,
            w_rank_up,
            gate_bias[None],
            decay_shift[None],
            out_gain[None],
            w_out.T,
        )
    ]
    own, l, r = pl.pallas_call(
        layer_kernel,
        out_shape=(jax.ShapeDtypeStruct(tokens.shape, F32),) + (jax.ShapeDtypeStruct(tokens.shape, BF16),) * 2,
        in_specs=[HBM] * 11,
        out_specs=(VMEM,) * 3,
        scratch_shapes=[
            pltpu.VMEM((128, D), BF16),
            pltpu.VMEM((NX, 2, 128, D), BF16),
            pltpu.VMEM((NZ, NY, 32, DK + DV), BF16),
            pltpu.VMEM((NZ, NY, 32, DK), BF16),
            pltpu.VMEM((NZ, NY, 32, DV), BF16),
            pltpu.VMEM((NX * QUAD, DK + DV), BF16),
            pltpu.VMEM((NX, QUAD, DK), F32),
            pltpu.VMEM((NX, 1, DK), F32),
            pltpu.VMEM((NX, DV, DK), BF16),
            pltpu.VMEM((NX * QUAD, DV), F32),
            pltpu.VMEM((NX * QUAD, DK), BF16),
            pltpu.VMEM((DV, DK), F32),
            pltpu.VMEM((64, 8, DK), BF16),
            pltpu.VMEM((1, DK), F32),
            pltpu.VMEM((64, 8, DK), BF16),
            pltpu.VMEM((64, 1, DK), F32),
            pltpu.VMEM((64, 8, DK), BF16),
            pltpu.VMEM((64, 8, DK), BF16),
            pltpu.VMEM((NX, 2, 128, D), BF16),
            pltpu.VMEM((NX, 128, D), BF16),
            pltpu.VMEM((3, 128, D), BF16),
            pltpu.VMEM((64, D), BF16),
            pltpu.VMEM((64, D), BF16),
            pltpu.VMEM((1, D), F32),
            pltpu.VMEM((16, D), BF16),
            pltpu.VMEM((16, DK), BF16),
            pltpu.VMEM((1, DK), F32),
            pltpu.VMEM((1, NX * QUAD), F32),
            pltpu.VMEM((1, DV), F32),
            pltpu.SemaphoreType.DMA((12,)),
            pltpu.SemaphoreType.DMA((14,)),
            pltpu.SemaphoreType.DMA((14,)),
            pltpu.SemaphoreType.DMA((2, 35)),
            pltpu.SemaphoreType.DMA((2, 35)),
            pltpu.SemaphoreType.DMA((4, 21)),
            pltpu.SemaphoreType.DMA((4, 21)),
            pltpu.SemaphoreType.DMA((3,)),
            pltpu.SemaphoreType.DMA((3,)),
            pltpu.SemaphoreType.DMA((10,)),
            pltpu.SemaphoreType.DMA((10,)),
        ],
        compiler_params=pltpu.CompilerParams(
            collective_id=0, has_side_effects=True, vmem_limit_bytes=40 * 1024 * 1024
        ),
    )(*inputs)
    return (own + l.astype(F32) + r.astype(F32)).astype(BF16)


def solution(mesh):
    finer = Mesh(mesh.devices.reshape(NZ, NY, NX, 2), ALL)
    in_specs = (
        P(ALL, None),
        P(),
        P(SP, TP),
        P(SP, TP),
        P(SP, TP),
        P(),
        P(None, TP),
        P(TP),
        P(SP),
        P(),
        P(TP, SP),
    )
    return jax.shard_map(on_device, mesh=finer, in_specs=in_specs, out_specs=P(ALL, None), check_vma=False)
```

```python
import jax
import jax.numpy as jnp
from jax import lax
from jax.experimental import pallas as pl
from jax.experimental.pallas import tpu as pltpu
from jax.sharding import Mesh
from jax.sharding import PartitionSpec as P

DK = 256
DV = 512
TAU = 16
BLOCK = 64
QUAD = 256
D = 2048
EPS = 1e-06
NY = NZ = 8
NX = 4
SP = ("z", "y")
TP = ("x", "c")
ALL = ("z", "y", "x", "c")
MESH = pl.DeviceIdType.MESH
VMEM = pl.BlockSpec(memory_space=pltpu.VMEM)
HBM = pl.BlockSpec(memory_space=pltpu.HBM)
BF16 = jnp.bfloat16
F32 = jnp.float32
NN, NT, TN = (((1,), (0,)), ((1,), (1,)), ((0,), (0,)))


def dot(a, b, dims):
    return lax.dot_general(a, b, (dims, ((), ())), preferred_element_type=F32)


def positions():
    return (lax.broadcasted_iota(jnp.int32, (QUAD, QUAD), i) for i in range(2))


def split3(value):
    hi = value.astype(BF16)
    rest = value - hi.astype(F32)
    mid = rest.astype(BF16)
    low = (rest - mid.astype(F32)).astype(BF16)
    return hi, mid, low


def remote(src, dst, send, recv, **device):
    return pltpu.make_async_remote_copy(
        src_ref=src, dst_ref=dst, send_sem=send, recv_sem=recv, device_id=device, device_id_type=MESH
    )


class Spread:
    def __init__(self, buf, at, rows, first, send, recv):
        self.buf, self.rows, self.send, self.recv = buf, rows, send, recv
        self.first, self.second = first, "z" if first == "y" else "y"
        self.at = at
        self.where = {"y": lax.axis_index("y"), "z": lax.axis_index("z")}

    def rest(self):
        return (pl.ds(self.at, self.rows), slice(None))

    def shard(self, along):
        pos = dict(self.where)
        pos[self.first] = along
        return self.buf.at[(pos["z"], pos["y"]) + self.rest()]

    def half(self, line, h):
        part = pl.ds(4 * h, 4)
        lead = (line, part) if self.second == "z" else (part, line)
        return self.buf.at[lead + self.rest()]

    def push(self, d):
        mine = self.where[self.first]
        ref = self.shard(mine)
        return remote(ref, ref, self.send.at[d - 1], self.recv.at[d - 1], **{self.first: lax.rem(mine + d, 8)})

    def start_push(self):
        for d in (1, 7, 2, 6, 3, 5, 4):
            self.push(d).start()

    def wait_push(self):
        mine = self.where[self.first]
        for d in (1, 7, 2, 6, 3, 5, 4):
            ref = self.shard(lax.rem(mine - d + 8, 8))
            remote(ref, ref, self.send.at[d - 1], self.recv.at[d - 1], **{self.first: mine}).wait_recv()

    def hop(self, s, h, way):
        mine = self.where[self.second]
        step = 1 if way == 0 else 7
        line = lax.rem(mine + (8 - step) * (s - 1), 8)
        ref = self.half(line, h)
        i = 7 + way * 7 + 2 * (s - 1) + (h if s < 4 else 0)
        return remote(ref, ref, self.send.at[i], self.recv.at[i], **{self.second: lax.rem(mine + step, 8)})

    def wait_hop(self, s, h, way):
        mine = self.where[self.second]
        step = 1 if way == 0 else 7
        ref = self.half(lax.rem(mine + (8 - step) * s, 8), h)
        i = 7 + way * 7 + 2 * (s - 1) + (h if s < 4 else 0)
        remote(ref, ref, self.send.at[i], self.recv.at[i], **{self.second: mine}).wait_recv()

    def hops(self, s):
        if s < 4:
            return [(0, 0), (1, 1), (1, 0), (0, 1)]
        return [(0, 0), (1, 1)]

    def finish(self):
        self.wait_hop(3, 1, 0)
        self.wait_hop(3, 0, 1)
        self.wait_hop(4, 0, 0)
        self.wait_hop(4, 1, 1)

    def drain(self):
        for d in range(1, 8):
            self.push(d).wait_send()
        for s in range(1, 5):
            for h, way in self.hops(s):
                self.hop(s, h, way).wait_send()


class FineSpread(Spread):
    def half(self, line, h):
        pair = lax.rem(lax.div(self.where[self.first], 2) + h, 4)
        part = pl.ds(2 * pair, 2)
        lead = (line, part) if self.second == "z" else (part, line)
        return self.buf.at[lead + self.rest()]

    def wait_from(self, d):
        mine = self.where[self.first]
        ref = self.shard(lax.rem(mine - d + 8, 8))
        remote(ref, ref, self.send.at[d - 1], self.recv.at[d - 1], **{self.first: mine}).wait_recv()

    def wait_pair(self, h):
        mine = self.where[self.first]
        odd = lax.rem(mine, 2)
        if h == 0:
            self.wait_from(7 - 6 * odd)
        else:
            for d in range(2):
                self.wait_from(lax.rem(8 - 2 * h + odd - d, 8))

    def index(self, s, h, way):
        return 7 + 14 * way + 4 * (s - 1) + (h if s < 4 else h // 2)

    def hop(self, s, h, way):
        mine = self.where[self.second]
        step = 1 if way == 0 else 7
        ref = self.half(lax.rem(mine + (8 - step) * (s - 1), 8), h)
        i = self.index(s, h, way)
        return remote(ref, ref, self.send.at[i], self.recv.at[i], **{self.second: lax.rem(mine + step, 8)})

    def wait_hop(self, s, h, way):
        mine = self.where[self.second]
        step = 1 if way == 0 else 7
        ref = self.half(lax.rem(mine + (8 - step) * s, 8), h)
        i = self.index(s, h, way)
        remote(ref, ref, self.send.at[i], self.recv.at[i], **{self.second: mine}).wait_recv()

    def hops(self, s):
        both = [(0, 0), (0, 1), (1, 0), (1, 1), (3, 0), (3, 1), (2, 0), (2, 1)]
        return both if s < 4 else [(0, 0), (1, 1), (2, 0), (3, 1)]

    def finish(self):
        for h in range(4):
            self.wait_hop(3, h, 1 - h % 2)
            self.wait_hop(4, h, h % 2)


def relay(pieces, s):
    for k in range(len(pieces[0].hops(s))):
        for p in pieces:
            h, way = p.hops(s)[k]
            if s > 1:
                p.wait_hop(s - 1, h, way)
            elif way == 0 and isinstance(p, FineSpread):
                p.wait_pair(h)
            p.hop(s, h, way).start()


def layer_kernel(
    tok_hbm,
    gain_hbm,
    wq_hbm,
    wk_hbm,
    wv_hbm,
    down_hbm,
    up_hbm,
    bias_hbm,
    shift_hbm,
    ogain_hbm,
    wo_hbm,
    own_ref,
    from_l,
    from_r,
    tok_ref,
    xn,
    wkv,
    wqb,
    wo,
    kv_ref,
    cum_ref,
    base_ref,
    starts,
    att_ref,
    far_ref,
    state_ref,
    give,
    got,
    decays,
    answer,
    carried,
    part,
    other,
    chip,
    ring_l,
    ring_r,
    gain_ref,
    down_ref,
    up_ref,
    bias_ref,
    shift_ref,
    ogain_ref,
    in_sem,
    tok_send,
    tok_recv,
    kv_send,
    kv_recv,
    w_send,
    w_recv,
    scan_send,
    scan_recv,
    rs_send,
    rs_recv,
):
    z, y, x, c = (lax.axis_index(a) for a in ALL)
    sp = z * NY + y
    right, left, mate = lax.rem(x + 1, NX), lax.rem(x + NX - 1, NX), 1 - c

    barrier = pltpu.get_barrier_semaphore()
    near = [{"x": right}, {"x": left}, {"c": mate}]
    near += [{a: lax.rem(i + d, 8)} for a, i in (("y", y), ("z", z)) for d in range(1, 8)]
    for device in near:
        pl.semaphore_signal(barrier, inc=1, device_id=device, device_id_type=MESH)

    loads = (
        pltpu.make_async_copy(wk_hbm, wkv.at[z, y, :, pl.ds(0, DK)], in_sem.at[0]),
        pltpu.make_async_copy(wv_hbm, wkv.at[z, y, :, pl.ds(DK, DV)], in_sem.at[1]),
        pltpu.make_async_copy(tok_hbm.at[pl.ds(0, 64)], tok_ref.at[pl.ds(0, 64)], in_sem.at[2]),
        pltpu.make_async_copy(tok_hbm.at[pl.ds(64, 64)], tok_ref.at[pl.ds(64, 64)], in_sem.at[3]),
        pltpu.make_async_copy(wq_hbm, wqb.at[z, y], in_sem.at[4]),
        pltpu.make_async_copy(wo_hbm, wo.at[z, y], in_sem.at[5]),
        pltpu.make_async_copy(gain_hbm, gain_ref, in_sem.at[6]),
        pltpu.make_async_copy(down_hbm, down_ref, in_sem.at[7]),
        pltpu.make_async_copy(up_hbm, up_ref, in_sem.at[8]),
        pltpu.make_async_copy(bias_hbm, bias_ref, in_sem.at[9]),
        pltpu.make_async_copy(shift_hbm, shift_ref, in_sem.at[10]),
        pltpu.make_async_copy(ogain_hbm, ogain_ref, in_sem.at[11]),
    )
    for load in loads:
        load.start()

    kv = tuple(FineSpread(wkv, 16 * i, 16, "yz"[i], kv_send.at[i], kv_recv.at[i]) for i in range(2))
    qs = tuple(Spread(wqb, 16 * i, 16, "yz"[i], w_send.at[i], w_recv.at[i]) for i in range(2))
    outs = tuple(Spread(wo, 16 * i, 16, "yz"[i], w_send.at[2 + i], w_recv.at[2 + i]) for i in range(2))

    def start_push(pieces):
        for p in pieces:
            p.start_push()

    def wait_push(pieces):
        for p in pieces:
            p.wait_push()

    def rows_of(xx, h):
        return xn.at[xx, c, pl.ds(64 * h, 64), :]

    def token(i, xx, h, to):
        ref = rows_of(xx, h)
        return remote(ref, ref, tok_send.at[i], tok_recv.at[i], x=to)

    def to_mate(i, xx, h):
        ref = rows_of(xx, h)
        return remote(ref, ref, tok_send.at[i], tok_recv.at[i], c=mate)

    def norm(h):
        rows = slice(64 * h, 64 * h + 64)
        wide = tok_ref[rows, :].astype(F32)
        normed = wide * lax.rsqrt(jnp.mean(wide * wide, axis=-1, keepdims=True) + EPS) * gain_ref[...]
        xn[x, c, rows, :] = normed.astype(BF16)

    far_x = lax.rem(x + 2, NX)
    sends = []

    def go(copy):
        copy.start()
        sends.append(copy)

    def arrive(i, xx, h, slot):
        token(i, xx, h, x).wait_recv()
        go(to_mate(slot, xx, h))

    def from_mate(i, xx, h):
        ref = xn.at[xx, mate, pl.ds(64 * h, 64), :]
        remote(ref, ref, tok_send.at[i], tok_recv.at[i], c=mate).wait_recv()

    row, col = positions()
    lower = jnp.where(col <= row, 1.0, 0.0).astype(BF16)

    def gates(i):
        rank = dot(xn[i].reshape(QUAD, D), down_ref[...], NT).astype(BF16)
        pre = dot(rank, up_ref[...], NN) + bias_ref[...]
        logs = jnp.minimum(pre, 0.0) - jnp.log1p(jnp.exp(-jnp.abs(pre)))
        hi, mid, low = split3(logs * (1.0 / TAU))
        cum_ref[i] = cum_ref[i] + (dot(lower, hi, NN) + (dot(lower, mid, NN) + dot(lower, low, NN)))

    def line_decay(d):
        ref = decays.at[z, y]
        return remote(ref, ref, scan_send.at[1], scan_recv.at[1], y=lax.rem(y + d, NY))

    def plane_decay(d):
        ref = decays.at[z]
        return remote(ref, ref, scan_send.at[3], scan_recv.at[3], z=lax.rem(z + d, NZ))

    def wait_decays(ref, sem):
        pltpu.make_async_copy(ref, ref, sem).wait()

    loads[0].wait()
    loads[1].wait()
    pl.semaphore_wait(barrier, 17)
    start_push(kv)
    loads[2].wait()
    loads[6].wait()
    norm(0)
    go(token(0, x, 0, right))
    go(to_mate(6, x, 0))
    loads[3].wait()
    norm(1)
    go(token(3, x, 1, left))
    go(to_mate(7, x, 1))
    go(token(1, x, 1, right))
    go(token(4, x, 0, left))
    loads[10].wait()
    for i in range(NX):
        shift = jnp.broadcast_to(shift_ref[:, i * QUAD : (i + 1) * QUAD], (QUAD, QUAD))
        hi, mid, low = split3(shift)
        cum_ref[i] = dot(lower, hi, NT) + (dot(lower, mid, NT) + dot(lower, low, NT))
    relay(kv, 1)
    from_mate(6, x, 0)
    from_mate(7, x, 1)
    for load in loads[7:10] + loads[11:]:
        load.wait()
    gates(x)
    relay(kv, 2)
    arrive(0, left, 0, 8)
    go(token(2, left, 0, right))
    arrive(3, right, 1, 9)
    go(token(5, right, 1, left))
    relay(kv, 3)
    arrive(1, left, 1, 10)
    arrive(4, right, 0, 11)
    loads[4].wait()
    start_push(qs)
    relay(kv, 4)
    loads[5].wait()
    start_push(outs)
    wait_push(qs)
    relay(qs, 1)
    from_mate(8, left, 0)
    from_mate(10, left, 1)
    gates(left)
    from_mate(9, right, 1)
    from_mate(11, right, 0)
    gates(right)
    arrive(2, far_x, 0, 12)
    arrive(5, far_x, 1, 13)
    relay(qs, 2)
    from_mate(12, far_x, 0)
    from_mate(13, far_x, 1)
    gates(far_x)
    base = jnp.zeros((1, DK), F32)
    for i in range(NX):
        base_ref[i] = base
        base = base + cum_ref[i, QUAD - 1 : QUAD]
    decays[z, y] = jnp.exp(base)
    for d in range(1, NY):
        line_decay(d).start()
    for p in kv:
        p.finish()

    state_ref[...] = jnp.zeros_like(state_ref)

    def absorb(i, carry):
        @pl.when(i == 0)
        def _():
            relay(qs, 3)
            wait_push(outs)
            relay(outs, 1)

        @pl.when(i == 2)
        def _():
            relay(qs, 4)

        @pl.when(i == 2)
        def _():
            wait_decays(decays.at[0, pl.ds(0, NY - 1)], scan_recv.at[1])
            for d in range(1, NZ):
                plane_decay(d).start()

        now = dot(xn[i].reshape(QUAD, D), wkv[...].reshape(D, DK + DV), NN).astype(BF16)
        kv_ref[pl.ds(pl.multiple_of(i * QUAD, QUAD), QUAD), :] = now
        cum = cum_ref[i]
        final = cum[QUAD - 1 : QUAD]
        decayed = (now[:, 0:DK].astype(F32) * jnp.exp(final - cum)).astype(BF16)
        state = state_ref[...]
        starts[i] = state.astype(BF16)
        state_ref[...] = jnp.exp(final) * state + dot(now[:, DK:], decayed, TN)
        return carry

    lax.fori_loop(0, NX, absorb, 0)

    give[...] = state_ref[...].reshape(64, 8, DK).astype(BF16)

    columns = [lax.rem(y + d, NY) for d in range(NY)]

    def ask(zz, yy):
        remote(give.at[zz * NY + yy], got.at[sp], scan_send.at[0], scan_recv.at[0], z=zz, y=yy).start()

    def reply(zz, yy):
        remote(answer.at[zz * NY + yy], carried.at[sp], scan_send.at[2], scan_recv.at[2], z=zz, y=yy).start()

    def to_all(send):
        def line(d, carry):
            zz = lax.rem(z + d, NZ)
            for yy in columns:
                send(zz, yy)
            return carry

        for yy in columns[1:]:
            send(z, yy)
        lax.fori_loop(1, NZ, line, 0)

    def wait_all(ref, sem):
        most = ref.at[pl.ds(0, 63)]
        pltpu.make_async_copy(most, most, sem).wait()

    relay(outs, 2)
    to_all(ask)
    got[sp] = give[sp]

    def attend(i, carry):
        at = pl.ds(pl.multiple_of(i * QUAD, QUAD), QUAD)
        q = dot(xn[i].reshape(QUAD, D), wqb[...].reshape(D, DK), NN).astype(BF16).astype(F32) * DK ** (-0.5)
        k = kv_ref[at, 0:DK].astype(F32)
        v = kv_ref[at, DK : DK + DV]
        cum = cum_ref[i]
        cube = cum.reshape(QUAD // BLOCK, BLOCK, DK)
        centre = (cube - cube[:, BLOCK // 2 : BLOCK // 2 + 1]).reshape(QUAD, DK)
        q_scaled = (q * jnp.exp(centre)).astype(BF16)
        k_scaled = (k * jnp.exp(-centre)).astype(BF16)
        causal = (row // BLOCK == col // BLOCK) & (col <= row)
        scores = jnp.where(causal, dot(q_scaled, k_scaled, NT), 0.0)
        lines = [scores[0:BLOCK]]
        for n in range(1, QUAD // BLOCK):
            cut = n * BLOCK
            edge = cum[cut - 1 : cut]
            q_part = (q[cut : cut + BLOCK] * jnp.exp(cum[cut : cut + BLOCK] - edge)).astype(BF16)
            k_part = (k[0:cut] * jnp.exp(edge - cum[0:cut])).astype(BF16)
            k_part = jnp.concatenate([k_part, jnp.zeros((QUAD - cut, DK), BF16)], axis=0)
            lines.append(scores[cut : cut + BLOCK] + dot(q_part, k_part, NT))
        scores = jnp.concatenate(lines, axis=0).astype(BF16)
        reach = q * jnp.exp(cum)
        att_ref[at, :] = dot(scores, v, NN) + dot(reach.astype(BF16), starts[i], NT)
        far_ref[at, :] = (reach * jnp.exp(base_ref[i])).astype(BF16)
        return carry

    for p in qs:
        p.finish()
    lax.fori_loop(0, 2, attend, 0)
    relay(outs, 3)
    lax.fori_loop(2, NX, attend, 0)
    wait_all(got, scan_recv.at[0])
    wait_decays(decays.at[pl.ds(0, NZ - 1)], scan_recv.at[3])

    def prefix(j, carry):
        answer[j] = carry.astype(BF16)
        return decays[lax.div(j, NY), lax.rem(j, NY)] * carry + got[j].astype(F32)

    lax.fori_loop(0, 64, prefix, jnp.zeros((8, DK), F32))
    to_all(reply)
    relay(outs, 4)
    for p in outs:
        p.finish()
    carried[sp] = answer[sp]
    wait_all(carried, scan_recv.at[2])

    halves = (pl.ds(0, 64), pl.ds(64, 64))

    def swap(k):
        return remote(part.at[k, mate], other.at[k], rs_send.at[k], rs_recv.at[k], c=mate)

    def ring(i, src, dst, to):
        return remote(src, dst, rs_send.at[4 + i], rs_recv.at[4 + i], x=to)

    hops = (
        ring(0, chip.at[0, halves[0]], ring_l, right),
        ring(1, chip.at[0, halves[1]], ring_r, left),
        ring(2, chip.at[1, halves[1]], from_l.at[halves[1]], right),
        ring(3, chip.at[2, halves[0]], from_r.at[halves[0]], left),
        ring(4, chip.at[1, halves[0]], from_l.at[halves[0]], right),
        ring(5, chip.at[2, halves[1]], from_r.at[halves[1]], left),
    )

    def both(k, rows):
        return part[k, c, rows, :].astype(F32) + other[k, rows, :].astype(F32)

    def finish(k, carry):
        off = jnp.where(k == 0, 2, jnp.where(k == 1, 1, jnp.where(k == 2, 3, 0)))
        to = lax.rem(x + off, NX)
        at = pl.ds(pl.multiple_of(to * QUAD, QUAD), QUAD)
        att = att_ref[at, :] + dot(far_ref[at, :], carried[...].reshape(DV, DK), NT)
        shaped = att * lax.rsqrt(jnp.mean(att * att, axis=-1, keepdims=True) + EPS) * ogain_ref[...]
        res = dot(shaped.astype(BF16), wo[...].reshape(D, DV), NT).astype(BF16)
        part[k] = res.reshape(2, 128, D)
        swap(k).start()

        @pl.when(k == 1)
        def _():
            swap(0).wait_recv()
            chip[0] = both(0, slice(None)).astype(BF16)
            hops[0].start()
            hops[1].start()

        @pl.when(k == 2)
        def _():
            swap(1).wait_recv()
            chip[1, halves[1], :] = both(1, halves[1]).astype(BF16)
            hops[2].start()

        @pl.when(k == 3)
        def _():
            swap(2).wait_recv()
            chip[2, halves[0], :] = both(2, halves[0]).astype(BF16)
            hops[3].start()

        return carry

    lax.fori_loop(0, NX, finish, 0)
    hops[0].wait_recv()
    chip[1, halves[0], :] = (both(1, halves[0]) + ring_l[...].astype(F32)).astype(BF16)
    hops[4].start()
    hops[1].wait_recv()
    chip[2, halves[1], :] = (both(2, halves[1]) + ring_r[...].astype(F32)).astype(BF16)
    hops[5].start()
    swap(3).wait_recv()
    for i in (2, 3, 4, 5):
        hops[i].wait_recv()
    own_ref[...] = both(3, slice(None))

    for s in sends:
        s.wait_send()
    for p in kv + qs + outs:
        p.drain()
    sent = give.at[pl.ds(0, 63)]
    pltpu.make_async_copy(sent, sent, scan_send.at[0]).wait()
    wait_decays(decays.at[0, pl.ds(0, NY - 1)], scan_send.at[1])
    wait_decays(decays.at[pl.ds(0, NZ - 1)], scan_send.at[3])
    wait_all(answer, scan_send.at[2])
    for k in range(4):
        swap(k).wait_send()
    for h in hops:
        h.wait_send()


def on_device(
    tokens,
    norm_gain,
    w_query,
    w_key,
    w_value,
    w_rank_down,
    w_rank_up,
    gate_bias,
    decay_shift,
    out_gain,
    w_out,
):
    inputs = [
        pltpu.with_memory_space_constraint(a, pltpu.HBM)
        for a in (
            tokens,
            norm_gain[None],
            w_query,
            w_key,
            w_value,
            w_rank_down.T,
            w_rank_up,
            gate_bias[None],
            decay_shift[None],
            out_gain[None],
            w_out.T,
        )
    ]
    own, l, r = pl.pallas_call(
        layer_kernel,
        out_shape=(jax.ShapeDtypeStruct(tokens.shape, F32),) + (jax.ShapeDtypeStruct(tokens.shape, BF16),) * 2,
        in_specs=[HBM] * 11,
        out_specs=(VMEM,) * 3,
        scratch_shapes=[
            pltpu.VMEM((128, D), BF16),
            pltpu.VMEM((NX, 2, 128, D), BF16),
            pltpu.VMEM((NZ, NY, 32, DK + DV), BF16),
            pltpu.VMEM((NZ, NY, 32, DK), BF16),
            pltpu.VMEM((NZ, NY, 32, DV), BF16),
            pltpu.VMEM((NX * QUAD, DK + DV), BF16),
            pltpu.VMEM((NX, QUAD, DK), F32),
            pltpu.VMEM((NX, 1, DK), F32),
            pltpu.VMEM((NX, DV, DK), BF16),
            pltpu.VMEM((NX * QUAD, DV), F32),
            pltpu.VMEM((NX * QUAD, DK), BF16),
            pltpu.VMEM((DV, DK), F32),
            pltpu.VMEM((64, 8, DK), BF16),
            pltpu.VMEM((64, 8, DK), BF16),
            pltpu.VMEM((NZ, NY, 1, DK), F32),
            pltpu.VMEM((64, 8, DK), BF16),
            pltpu.VMEM((64, 8, DK), BF16),
            pltpu.VMEM((NX, 2, 128, D), BF16),
            pltpu.VMEM((NX, 128, D), BF16),
            pltpu.VMEM((3, 128, D), BF16),
            pltpu.VMEM((64, D), BF16),
            pltpu.VMEM((64, D), BF16),
            pltpu.VMEM((1, D), F32),
            pltpu.VMEM((16, D), BF16),
            pltpu.VMEM((16, DK), BF16),
            pltpu.VMEM((1, DK), F32),
            pltpu.VMEM((1, NX * QUAD), F32),
            pltpu.VMEM((1, DV), F32),
            pltpu.SemaphoreType.DMA((12,)),
            pltpu.SemaphoreType.DMA((14,)),
            pltpu.SemaphoreType.DMA((14,)),
            pltpu.SemaphoreType.DMA((2, 35)),
            pltpu.SemaphoreType.DMA((2, 35)),
            pltpu.SemaphoreType.DMA((4, 21)),
            pltpu.SemaphoreType.DMA((4, 21)),
            pltpu.SemaphoreType.DMA((4,)),
            pltpu.SemaphoreType.DMA((4,)),
            pltpu.SemaphoreType.DMA((10,)),
            pltpu.SemaphoreType.DMA((10,)),
        ],
        compiler_params=pltpu.CompilerParams(
            collective_id=0, has_side_effects=True, vmem_limit_bytes=40 * 1024 * 1024
        ),
    )(*inputs)
    return (own + l.astype(F32) + r.astype(F32)).astype(BF16)


def solution(mesh):
    finer = Mesh(mesh.devices.reshape(NZ, NY, NX, 2), ALL)
    in_specs = (
        P(ALL, None),
        P(),
        P(SP, TP),
        P(SP, TP),
        P(SP, TP),
        P(),
        P(None, TP),
        P(TP),
        P(SP),
        P(),
        P(TP, SP),
    )
    return jax.shard_map(on_device, mesh=finer, in_specs=in_specs, out_specs=P(ALL, None), check_vma=False)
```
